512 devices in a mesh: ep: 32 (over z, core), tp: 16 (over y, x).
Axes of the slice: x: 4, y: 4, z: 16, core: 2. Of those that a mesh axis runs over, the one named last changes fastest.
Arguments:
- tokens: bfloat16 [4096, 2048], P('ep'), may hold values from -6 to 6
- cotangent: bfloat16 [4096, 2048], P('ep'), may hold values from -6 to 6
- expert_ids: int32 [4096, 2], P('ep'), may hold values from 0 to 31, all different within a row; in each aligned block of 128 rows (0 to 127, 128 to 255, ...) at most 16 rows name the same one
- route_weight: bfloat16 [4096, 2], P('ep'), may hold values from 0.19921875 to 1
- gate_weight: bfloat16 [32, 1024, 2048], P('ep', 'tp'), may hold values from -0.125 to 0.125
- up_weight: bfloat16 [32, 1024, 2048], P('ep', 'tp'), may hold values from -0.125 to 0.125
- down_weight: bfloat16 [32, 1024, 2048], P('ep', 'tp'), may hold values from -0.1875 to 0.1875
Outputs:
- tokens_grad: bfloat16 [4096, 2048], P('ep', 'tp')
- route_weight_grad: float32 [4096, 2], P('ep')
- gate_weight_grad: float32 [32, 1024, 2048], P('ep', 'tp')
- up_weight_grad: float32 [32, 1024, 2048], P('ep', 'tp')
- down_weight_grad: float32 [32, 1024, 2048], P('ep', 'tp')
The draws below stay inside these ranges and needn't reach their ends.
Inputs may be any that keep to these rules, and one draw needn't show every extreme that they name: `expert_ids`: within each aligned block of 128 rows every expert is named at most 16 times; the two experts of a row differ.
All inputs are finite; a program needn't handle non-finite values.
Results may differ from the reference program's by a relative error of at most 0.0058.
Values may be sent and summed in bfloat16 or wider, within the bound.
No kernel may reach another device: no remote copies, remote signals or barrier semaphores. Data moves between devices by JAX's collectives and lax.ppermute only.
A program may use at most 64 MiB of HBM per device.

```python
import math
import jax
import jax.numpy as jnp
import numpy as np
from jax import lax

D = 2048
FE = 1024
TOP = 2
TOK_DEV = 128
EXPERTS = 32
TOKENS = 4096
CAP = 16
N_EP = 32


def block_scale(rng, shape, split, smallest, high):
    loudness, own = 1.0, jax.random.fold_in(rng, 6)
    for axis_at, parts in split:
        draws = jnp.exp(jax.random.uniform(jax.random.fold_in(own, axis_at), (parts,), jnp.float32, smallest / len(split), high / len(split)))
        loudness = loudness * jnp.repeat(draws, shape[axis_at] // parts).reshape([-1 if axis == axis_at else 1 for axis in range(len(shape))])
    return loudness


def assign_block(own_key, own, number, rows, count, top, most, slope):
    sequence = jax.random.permutation(own_key, count)
    crowded, common = load_shares(count, rows * top, most, slope, True), load_shares(count, rows * top, most, slope, False)
    places = jnp.arange(count)

    def named(tallies, turn):
        used = int((tallies > 0).sum())
        fixed = max(1, used // 4)
        shifted = fixed + (places - fixed + turn * (used - fixed)) % max(1, count - fixed)
        return jnp.zeros((count,), jnp.int32).at[sequence[jnp.where(places < fixed, places, shifted)]].set(jnp.asarray(tallies, jnp.int32))

    tallies = jnp.where(number % 4 == 0, named(crowded, number // 4), named(common, number - number // 4 - 1))
    mixed = jax.random.permutation(jax.random.fold_in(own, 3), count)
    source_of, taker = mixed[0:count // 2 * 2:2], mixed[1:count // 2 * 2:2]
    slack = jnp.minimum(tallies[source_of] - 1, most - tallies[taker]) // 2
    slack = jnp.where((source_of == sequence[0]) | (taker == sequence[0]) | (tallies[taker] == 0), 0, jnp.maximum(slack, 0))
    shifted = jax.random.randint(jax.random.fold_in(own, 4), (count // 2,), 0, 1 << 20) % (slack + 1)
    tallies = tallies.at[source_of].add(-shifted).at[taker].add(shifted)
    items = jnp.searchsorted(jnp.cumsum(tallies), jnp.arange(rows * top), side="right").astype(jnp.int32)
    listing = items.reshape(top, rows).T
    listing = listing[jax.random.permutation(jax.random.fold_in(own, 1), rows)]
    turn = jax.random.randint(jax.random.fold_in(own, 2), (rows, 1), 0, top)
    return jnp.take_along_axis(listing, (jnp.arange(top)[None, :] + turn) % top, axis=1)


def load_shares(amount, total, most, slope, full):
    portions = [(1 << 20) // math.isqrt(rank ** slope) + 1 for rank in range(1, amount + 1)]
    largest = most if full else min(most, max(-(-total // amount), total * portions[0] // sum(portions)))
    least = 1 if total - largest >= amount - 1 else 0
    given, spare = [largest] + [least] * (amount - 1), total - largest - least * (amount - 1)
    while spare > 0:
        free = [i for i in range(1, amount) if given[i] < largest] or [i for i in range(1, amount) if given[i] < most]
        whole, left = sum([portions[i] for i in free]), spare
        for i in free:
            extra = min(most - given[i], max(1, left * portions[i] // whole), spare)
            given[i] = given[i] + extra
            spare = spare - extra
    return np.array(given)


def gaussian(stream_key, shape, spread, reach, cuts=(), kind=jnp.bfloat16):
    entries = spread * jax.random.normal(stream_key, shape, jnp.float32)
    if cuts:
        entries = entries * block_scale(stream_key, shape, cuts, -0.22, 0.18)
    return jnp.clip(entries, -reach, reach).astype(kind)


def setup_inputs(seed: int = 0) -> dict:
    streams_of = jax.random.split(jax.random.key(seed), 8)
    tokens = gaussian(streams_of[0], (TOKENS, D), 1.0, 6.0, ((0, 32),))
    cotangent = gaussian(streams_of[1], (TOKENS, D), 1.0, 6.0, ((0, 32),))
    expert_ids_keys = jax.random.split(jax.random.fold_in(streams_of[2], 1), TOKENS // TOK_DEV)
    expert_ids_turns = jax.random.permutation(jax.random.fold_in(streams_of[2], 3), TOKENS // TOK_DEV)
    expert_ids = jax.vmap(lambda own, number: assign_block(jax.random.fold_in(streams_of[2], 2), own, number, TOK_DEV, EXPERTS, TOP, CAP, 2))(expert_ids_keys, expert_ids_turns).reshape((TOKENS, TOP))
    route_weight = jnp.clip(0.19921875 + 0.80078125 * jax.random.uniform(streams_of[3], (TOKENS, TOP), jnp.float32) ** block_scale(streams_of[3], (TOKENS, TOP), ((0, 32),), -0.2, 0.2), 0.19921875, 1.0).astype(jnp.bfloat16)
    gate_weight = gaussian(streams_of[4], (EXPERTS, FE, D), D ** -0.5, 0.125, ((0, 32), (1, 16)))
    up_weight = gaussian(streams_of[5], (EXPERTS, FE, D), D ** -0.5, 0.125, ((0, 32), (1, 16)))
    down_weight = gaussian(streams_of[6], (EXPERTS, FE, D), FE ** -0.5, 0.1875, ((0, 32), (1, 16)))
    return {"tokens": tokens, "cotangent": cotangent, "expert_ids": expert_ids, "route_weight": route_weight, "gate_weight": gate_weight, "up_weight": up_weight, "down_weight": down_weight}


def reference(tokens, cotangent, expert_ids, route_weight, gate_weight, up_weight, down_weight):
    routed = TOKENS * TOP
    buffer_rows = N_EP * CAP
    flat_ids = expert_ids.reshape(-1)
    flat_weight = route_weight.reshape(-1)

    def one_expert(expert):
        picked = jnp.nonzero(flat_ids == expert, size=buffer_rows, fill_value=routed)[0].astype(jnp.int32)
        usable = picked < routed
        safe_pair = jnp.minimum(picked, routed - 1)
        token_of = safe_pair // TOP
        routed_rows = tokens[token_of]
        routed_cotangent = cotangent[token_of]
        weight = jnp.where(usable, flat_weight[safe_pair].astype(jnp.float32), jnp.float32(0.0))[:, None]
        gate_w = lax.dynamic_index_in_dim(gate_weight, expert, 0, keepdims=False)
        up_w = lax.dynamic_index_in_dim(up_weight, expert, 0, keepdims=False)
        down_w = lax.dynamic_index_in_dim(down_weight, expert, 0, keepdims=False)
        pre_gate = jnp.dot(routed_rows, gate_w.T, preferred_element_type=jnp.float32)
        pre_up = jnp.dot(routed_rows, up_w.T, preferred_element_type=jnp.float32)
        sigma = jax.nn.sigmoid(pre_gate)
        silu_gate = pre_gate * sigma
        hidden = silu_gate * pre_up
        back_hidden = jnp.dot(routed_cotangent, down_w.T, preferred_element_type=jnp.float32)
        products = jnp.sum(hidden * back_hidden, axis=1)
        scaled = weight * back_hidden
        grad_gate = (scaled * pre_up * sigma * (1.0 + pre_gate * (1.0 - sigma))).astype(jnp.bfloat16)
        grad_up = (scaled * silu_gate).astype(jnp.bfloat16)
        weighted = (weight * hidden).astype(jnp.bfloat16)
        down_grad = jnp.dot(weighted.T, routed_cotangent, preferred_element_type=jnp.float32)
        gate_grad = jnp.dot(grad_gate.T, routed_rows, preferred_element_type=jnp.float32)
        up_grad = jnp.dot(grad_up.T, routed_rows, preferred_element_type=jnp.float32)
        pair_grad = (jnp.dot(grad_gate, gate_w, preferred_element_type=jnp.float32)
                     + jnp.dot(grad_up, up_w, preferred_element_type=jnp.float32)).astype(jnp.bfloat16)
        return gate_grad, up_grad, down_grad, picked, pair_grad, products

    gate_grad, up_grad, down_grad, picked, pair_grad, products = lax.map(
        one_expert, jnp.arange(EXPERTS, dtype=jnp.int32))
    slot_flat = picked.reshape(-1)
    token_sum = jnp.zeros((routed, D), jnp.float32).at[slot_flat].set(
        pair_grad.reshape(-1, D).astype(jnp.float32), mode="drop")
    tokens_grad = jnp.sum(token_sum.reshape(TOKENS, TOP, D), axis=1).astype(jnp.bfloat16)
    route_grad = jnp.zeros((routed,), jnp.float32).at[slot_flat].set(products.reshape(-1), mode="drop")
    return tokens_grad, route_grad.reshape(TOKENS, TOP), gate_grad, up_grad, down_grad
```

```python
import functools

import jax
import jax.numpy as jnp
from jax import lax
from jax.experimental import pallas as pl
from jax.experimental.pallas import tpu as pltpu
from jax.sharding import Mesh
from jax.sharding import PartitionSpec as P

BF = jnp.bfloat16
F32 = jnp.float32
I32 = jnp.int32
NZ = 16
TP = 16
TOK = 128
CAP = 16
COL = 128
HID = 64
ROWS = 512
BLK = 4
RB = ROWS // BLK
EXT = 8


def iota(shape, dim):
    return lax.broadcasted_iota(I32, shape, dim)


def dot(a, b, ca, cb, precision=None):
    return lax.dot_general(
        a, b, (((ca,), (cb,)), ((), ())), precision=precision, preferred_element_type=F32
    )


def routing(ids_ref, core):
    experts = 2 * NZ
    row = iota((experts, TOK), 0)
    first = (ids_ref[0:1, :] == row).astype(F32)
    second = (ids_ref[1:2, :] == row).astype(F32)
    member = first + second
    earlier = (iota((TOK, TOK), 0) < iota((TOK, TOK), 1)).astype(BF)
    rank = dot(member.astype(BF), earlier, 1, 0)
    slots = 2 * NZ * CAP
    slot = iota((slots, experts), 0)
    half = slot >> 8
    expert = 2 * ((slot & 255) >> 4) + jnp.where(half == 0, core, 1 - core)
    expand = (expert == iota((slots, experts), 1)).astype(BF)
    hit = dot(expand, member.astype(BF), 1, 0)
    at = dot(expand, rank.astype(BF), 1, 0)
    place = (iota((slots, TOK), 0) & 15).astype(F32)
    chosen = (hit > 0.5) & (at == place)
    return first, second, rank, expand, chosen


def dispatch_kernel(s_ref, ids_ref, w_ref, tok_ref, cot_ref, own_ref, other_ref):
    first, second, _, expand, chosen = routing(ids_ref, s_ref[1])
    w = w_ref[...].astype(F32)
    weighted = first * w[0:1, :] + second * w[1:2, :]
    scale = dot(expand, weighted.astype(BF), 1, 0)
    pick = jnp.where(chosen, 1.0, 0.0).astype(BF)
    pick_scaled = jnp.where(chosen, scale, 0.0).astype(BF)
    rows = dot(pick, tok_ref[...], 1, 0).astype(BF)
    cots = dot(pick_scaled, cot_ref[...], 1, 0).astype(BF)
    half = NZ * CAP
    own_ref[:, 0] = rows[:half].reshape(NZ, CAP, COL)
    own_ref[:, 1] = cots[:half].reshape(NZ, CAP, COL)
    other_ref[:, 0] = rows[half:].reshape(NZ, CAP, COL)
    other_ref[:, 1] = cots[half:].reshape(NZ, CAP, COL)


def dispatch(where, ids, w, tokens, cotangent):
    full = lambda *shape: pl.BlockSpec(shape, lambda i, s: (0,) * len(shape))
    out = jax.ShapeDtypeStruct((NZ, 2, CAP, COL), BF)
    return pl.pallas_call(
        dispatch_kernel,
        grid_spec=pltpu.PrefetchScalarGridSpec(
            num_scalar_prefetch=1,
            grid=(1,),
            in_specs=[
                full(2, TOK),
                full(2, TOK),
                pl.BlockSpec((TOK, COL), lambda i, s: (0, s[0])),
                pl.BlockSpec((TOK, COL), lambda i, s: (0, s[0])),
            ],
            out_specs=[full(NZ, 2, CAP, COL)] * 2,
        ),
        out_shape=[out, out],
        name="dispatch",
        cost_estimate=pl.CostEstimate(flops=10**8, bytes_accessed=10**6, transcendentals=0),
    )(where, ids, w, tokens, cotangent)


def forward_kernel(x_ref, wg_ref, wu_ref, wd_ref, part_ref, gg_ref, gu_ref, wt_ref, xt, xc):
    for j in range(TP):
        xt[:, j * COL : (j + 1) * COL] = x_ref[j, :, 0].reshape(RB, COL)
        xc[:, j * COL : (j + 1) * COL] = x_ref[j, :, 1].reshape(RB, COL)
    wg, wu = wg_ref[0], wu_ref[0]
    gate = dot(xt[...], wg, 1, 1)
    up = dot(xt[...], wu, 1, 1)
    back = dot(xc[...], wd_ref[0], 1, 1)
    sigma = 1.0 / (1.0 + jnp.exp(-gate))
    silu = gate * sigma
    hidden = silu * up
    grad_gate = (back * up * sigma * (1.0 + gate * (1.0 - sigma))).astype(BF)
    grad_up = (back * silu).astype(BF)
    gg_ref[...] = grad_gate
    gu_ref[...] = grad_up
    wt_ref[...] = hidden.astype(BF)
    total = jnp.sum(hidden * back, axis=1, keepdims=True)
    lane = iota((RB, COL), 1)
    spread = jnp.where((lane & 31) == (iota((RB, COL), 0) & 31), total, 0.0)
    group = (iota((EXT, RB), 0) == (iota((EXT, RB), 1) >> 5)).astype(F32)
    sums = dot(group, spread, 1, 0, lax.Precision.HIGHEST)
    high = sums.astype(BF)
    low = (sums - high.astype(F32)).astype(BF)
    extra = jnp.where(iota((EXT, COL), 1) < 32, high.astype(F32), low.astype(F32)).astype(BF)
    for j in range(TP):
        cols = slice(j * COL, (j + 1) * COL)
        piece = dot(grad_gate, wg[:, cols], 1, 0) + dot(grad_up, wu[:, cols], 1, 0)
        part_ref[j, 0, :RB] = piece.astype(BF)
        part_ref[j, 0, RB:] = extra


def forward(x, wg, wu, wd):
    d = TP * COL
    weight = pl.BlockSpec((1, HID, d), lambda i: (0, 0, 0))
    grads = pl.BlockSpec((RB, HID), lambda i: (i, 0))
    gs = jax.ShapeDtypeStruct((ROWS, HID), BF)
    return pl.pallas_call(
        forward_kernel,
        grid=(BLK,),
        in_specs=[
            pl.BlockSpec((TP, NZ // BLK, 2, 2 * CAP, COL), lambda i: (0, i, 0, 0, 0)),
            weight,
            weight,
            weight,
        ],
        out_specs=[
            pl.BlockSpec((TP, 1, RB + EXT, COL), lambda i: (0, i, 0, 0)),
            grads,
            grads,
            grads,
        ],
        out_shape=[jax.ShapeDtypeStruct((TP, BLK, RB + EXT, COL), BF), gs, gs, gs],
        scratch_shapes=[pltpu.VMEM((RB, d), BF), pltpu.VMEM((RB, d), BF)],
        name="forward",
        cost_estimate=pl.CostEstimate(flops=7 * 10**8, bytes_accessed=7 * 10**6, transcendentals=10**5),
    )(x, wg, wu, wd)


def weights_kernel(x_ref, gg_ref, gu_ref, wt_ref, dg_ref, du_ref, dd_ref):
    gg, gu, wt = gg_ref[...], gu_ref[...], wt_ref[...]
    for j in range(x_ref.shape[0]):
        cols = slice(j * COL, (j + 1) * COL)
        rows = x_ref[j, :, 0].reshape(ROWS, COL)
        cots = x_ref[j, :, 1].reshape(ROWS, COL)
        dg_ref[0, :, cols] = dot(gg, rows, 0, 0)
        du_ref[0, :, cols] = dot(gu, rows, 0, 0)
        dd_ref[0, :, cols] = dot(wt, cots, 0, 0)


def weights(x, gg, gu, wt):
    d, pieces = TP * COL, 4
    out = jax.ShapeDtypeStruct((1, HID, d), F32)
    grads = pl.BlockSpec((ROWS, HID), lambda i: (0, 0))
    return pl.pallas_call(
        weights_kernel,
        grid=(TP // pieces,),
        in_specs=[
            pl.BlockSpec((pieces, NZ, 2, 2 * CAP, COL), lambda i: (i, 0, 0, 0, 0)),
            grads,
            grads,
            grads,
        ],
        out_specs=[pl.BlockSpec((1, HID, pieces * COL), lambda i: (0, 0, i))] * 3,
        out_shape=[out, out, out],
        name="weights",
        cost_estimate=pl.CostEstimate(flops=4 * 10**9, bytes_accessed=6 * 10**6, transcendentals=0),
    )(x, gg, gu, wt)


def total_kernel(p_ref, out_ref):
    rows = p_ref[0, 0].astype(F32)
    for j in range(1, TP):
        rows = rows + p_ref[j, 0].astype(F32)
    out_ref[:, : 2 * CAP] = rows[:RB].astype(BF).reshape(NZ // BLK, 2 * CAP, COL)
    sums = rows[RB:]
    sums = sums + pltpu.roll(sums, COL - 32, 1)
    high = sums.astype(BF).astype(F32)
    low = pltpu.roll(sums - high, 32, 1)
    extra = jnp.where(iota((EXT, COL), 1) < 32, high, low)
    for k in range(NZ // BLK):
        out_ref[k, 2 * CAP :] = jnp.broadcast_to(extra[k : k + 1], (EXT, COL)).astype(BF)


def total(part):
    return pl.pallas_call(
        total_kernel,
        grid=(BLK,),
        in_specs=[pl.BlockSpec((TP, 1, RB + EXT, COL), lambda i: (0, i, 0, 0))],
        out_specs=pl.BlockSpec((NZ // BLK, 2 * CAP + EXT, COL), lambda i: (i, 0, 0)),
        out_shape=jax.ShapeDtypeStruct((NZ, 2 * CAP + EXT, COL), BF),
        name="total",
        cost_estimate=pl.CostEstimate(flops=10**7, bytes_accessed=2 * 10**6, transcendentals=0),
    )(part)


def combine_kernel(s_ref, ids_ref, w_ref, own_ref, other_ref, tok_ref, route_ref):
    core = s_ref[1]
    first, second, rank, _, chosen = routing(ids_ref, core)
    pick = jnp.where(chosen, 1.0, 0.0).astype(BF)
    half = NZ * CAP
    own = own_ref[:, :CAP].reshape(half, COL)
    other = other_ref[:, :CAP].reshape(half, COL)
    tok_ref[...] = (dot(pick[:half], own, 0, 0) + dot(pick[half:], other, 0, 0)).astype(BF)
    own_sums = own_ref[:, 2 * CAP :].reshape(NZ * EXT, COL)
    other_sums = other_ref[:, CAP:].reshape(NZ * EXT, COL)
    row = iota((NZ * EXT, TOK), 0)
    leads = (row & 7) == 0
    chip = row >> 3
    lane = iota((COL, TOK), 0)
    w = w_ref[...].astype(F32)
    for k, member in enumerate((first, second)):
        ids = ids_ref[k : k + 1, :]
        at = jnp.sum(member * rank, axis=0, keepdims=True).astype(I32)
        mine = (leads & (ids == 2 * chip + core)).astype(BF)
        theirs = (leads & (ids == 2 * chip + 1 - core)).astype(BF)
        near = dot(own_sums, mine, 0, 0)
        far = dot(other_sums, theirs, 0, 0)
        near = jnp.where((lane == at) | (lane == at + 32), near, 0.0)
        far = jnp.where((lane == at + 16) | (lane == at + 48), far, 0.0)
        route_ref[k : k + 1, :] = jnp.sum(near + far, axis=0, keepdims=True) / w[k : k + 1, :]


def combine(where, ids, w, own, other):
    full = lambda *shape: pl.BlockSpec(shape, lambda i, s: (0,) * len(shape))
    return pl.pallas_call(
        combine_kernel,
        grid_spec=pltpu.PrefetchScalarGridSpec(
            num_scalar_prefetch=1,
            grid=(1,),
            in_specs=[
                full(2, TOK),
                full(2, TOK),
                full(NZ, 2 * CAP + EXT, COL),
                full(NZ, CAP + EXT, COL),
            ],
            out_specs=[full(TOK, COL), full(2, TOK)],
        ),
        out_shape=[jax.ShapeDtypeStruct((TOK, COL), BF), jax.ShapeDtypeStruct((2, TOK), F32)],
        name="combine",
        cost_estimate=pl.CostEstimate(flops=10**8, bytes_accessed=10**6, transcendentals=0),
    )(where, ids, w, own, other)


def exchange(x, axis):
    return lax.all_to_all(x, axis, split_axis=0, concat_axis=0, tiled=True)


def per_device(tokens, cotangent, expert_ids, route_weight, gate_weight, up_weight, down_weight):
    swap = [(0, 1), (1, 0)]
    tp = lax.axis_index("y") * lax.axis_size("x") + lax.axis_index("x")
    where = jnp.stack([tp, lax.axis_index("c")]).astype(I32)
    ids, w = expert_ids.T, route_weight.T
    own, other = dispatch(where, ids, w, tokens, cotangent)
    got = lax.ppermute(other, "c", swap)
    mine = jnp.stack([own, got], axis=2).reshape(NZ, 2, 2 * CAP, COL)
    mine = exchange(mine, "z")
    gathered = exchange(jnp.broadcast_to(mine[None], (TP, *mine.shape)), ("y", "x"))
    part, gg, gu, wt = forward(gathered, gate_weight, up_weight, down_weight)
    parts = exchange(part, ("y", "x"))
    gate_grad, up_grad, down_grad = weights(gathered, gg, gu, wt)
    back = exchange(total(parts), "z")
    far = lax.ppermute(back[:, CAP:], "c", swap)
    tokens_grad, route_grad = combine(where, ids, w, back, far)
    return tokens_grad, route_grad.T, gate_grad, up_grad, down_grad


def solution(mesh):
    grid = Mesh(mesh.devices.reshape(NZ, 2, 4, 4), ("z", "c", "y", "x"))
    ep, tp = ("z", "c"), ("y", "x")
    weight = P(ep, tp, None)
    return jax.shard_map(
        per_device,
        mesh=grid,
        in_specs=(P(ep, None), P(ep, None), P(ep, None), P(ep, None), weight, weight, weight),
        out_specs=(P(ep, tp), P(ep, None), weight, weight, weight),
        check_vma=False,
    )
```

```python
import jax
import jax.numpy as jnp
from jax import lax
from jax.experimental import pallas as pl
from jax.experimental.pallas import tpu as pltpu
from jax.sharding import Mesh
from jax.sharding import PartitionSpec as P


BF = jnp.bfloat16
F32 = jnp.float32
I32 = jnp.int32
NZ = 16
TP = 16
TOK = 128
CAP = 16
COL = 128
HID = 64
ROWS = 512
BLK = 4
RB = ROWS // BLK
EXT = 8


def iota(shape, dim):
    return lax.broadcasted_iota(I32, shape, dim)


def dot(a, b, ca, cb, precision=None):
    return lax.dot_general(
        a, b, (((ca,), (cb,)), ((), ())), precision=precision, preferred_element_type=F32
    )


def routing(ids_ref, core):
    experts = 2 * NZ
    row = iota((experts, TOK), 0)
    first = (ids_ref[0:1, :] == row).astype(F32)
    second = (ids_ref[1:2, :] == row).astype(F32)
    member = first + second
    earlier = (iota((TOK, TOK), 0) < iota((TOK, TOK), 1)).astype(BF)
    rank = dot(member.astype(BF), earlier, 1, 0)
    slots = 2 * NZ * CAP
    slot = iota((slots, experts), 0)
    half = slot >> 8
    expert = 2 * ((slot & 255) >> 4) + jnp.where(half == 0, core, 1 - core)
    expand = (expert == iota((slots, experts), 1)).astype(BF)
    hit = dot(expand, member.astype(BF), 1, 0)
    at = dot(expand, rank.astype(BF), 1, 0)
    place = (iota((slots, TOK), 0) & 15).astype(F32)
    chosen = (hit > 0.5) & (at == place)
    return first, second, rank, expand, chosen


def dispatch_kernel(s_ref, ids_ref, w_ref, tok_ref, cot_ref, own_ref, other_ref):
    first, second, _, expand, chosen = routing(ids_ref, s_ref[1])
    w = w_ref[...].astype(F32)
    weighted = first * w[0:1, :] + second * w[1:2, :]
    scale = dot(expand, weighted.astype(BF), 1, 0)
    pick = jnp.where(chosen, 1.0, 0.0).astype(BF)
    pick_scaled = jnp.where(chosen, scale, 0.0).astype(BF)
    rows = dot(pick, tok_ref[...], 1, 0).astype(BF)
    cots = dot(pick_scaled, cot_ref[...], 1, 0).astype(BF)
    half = NZ * CAP
    own_ref[:, 0] = rows[:half].reshape(NZ, CAP, COL)
    own_ref[:, 1] = cots[:half].reshape(NZ, CAP, COL)
    other_ref[:, 0] = rows[half:].reshape(NZ, CAP, COL)
    other_ref[:, 1] = cots[half:].reshape(NZ, CAP, COL)


def dispatch(where, ids, w, tokens, cotangent):
    full = lambda *shape: pl.BlockSpec(shape, lambda i, s: (0,) * len(shape))
    out = jax.ShapeDtypeStruct((NZ, 2, CAP, COL), BF)
    return pl.pallas_call(
        dispatch_kernel,
        grid_spec=pltpu.PrefetchScalarGridSpec(
            num_scalar_prefetch=1,
            grid=(1,),
            in_specs=[
                full(2, TOK),
                full(2, TOK),
                pl.BlockSpec((TOK, COL), lambda i, s: (0, s[0])),
                pl.BlockSpec((TOK, COL), lambda i, s: (0, s[0])),
            ],
            out_specs=[full(NZ, 2, CAP, COL)] * 2,
        ),
        out_shape=[out, out],
        name="dispatch",
        cost_estimate=pl.CostEstimate(flops=10**8, bytes_accessed=10**6, transcendentals=0),
    )(where, ids, w, tokens, cotangent)


def forward_kernel(
    s_ref, t_ref, c0_ref, c1_ref, c2_ref, c3_ref, wg_ref, wu_ref, wd_ref, g_ref, wt_ref, xt, xc, wgu, wdd
):
    @pl.when(pl.program_id(0) == 0)
    def _():
        wgu[:HID] = wg_ref[0]
        wgu[HID:] = wu_ref[0]
        wdd[:HID] = wd_ref[0]
        wdd[HID:] = wd_ref[0]

    for j in range(TP):
        xt[:, j * COL : (j + 1) * COL] = t_ref[j].reshape(RB, COL)
    for kx, c_ref in enumerate((c0_ref, c1_ref, c2_ref, c3_ref)):
        for ky in range(4):
            xc[:, piece_cols(s_ref, kx, ky)] = c_ref[ky].reshape(RB, COL)
    pre = dot(xt[...], wgu[...], 1, 1)
    back = dot(xc[...], wdd[...], 1, 1)
    lane = iota((RB, COL), 1)
    low_half = lane < HID
    turned = pltpu.roll(pre, HID, 1)
    gate = jnp.where(low_half, pre, turned)
    up = jnp.where(low_half, turned, pre)
    sigma = 1.0 / (1.0 + jnp.exp(-gate))
    silu = gate * sigma
    hidden = silu * up
    grads = jnp.where(low_half, back * up * sigma * (1.0 + gate * (1.0 - sigma)), back * silu).astype(BF)
    wt_ref[...] = hidden[:, :HID].astype(BF)
    total = jnp.sum(jnp.where(low_half, hidden * back, 0.0), axis=1, keepdims=True)
    spread = jnp.where((lane & 31) == (iota((RB, COL), 0) & 31), total, 0.0)
    group = (iota((EXT, RB), 0) == (iota((EXT, RB), 1) >> 5)).astype(F32)
    extra = two_parts(dot(group, spread, 1, 0, lax.Precision.HIGHEST))
    for x in range(4):
        g_ref[x, 0, :RB] = grads
        g_ref[x, 0, RB:] = extra


def two_parts(sums):
    high = sums.astype(BF).astype(F32)
    return jnp.where(iota((EXT, COL), 1) < 32, high, sums - high).astype(BF)


def one_sum(parts):
    both = parts + pltpu.roll(parts, COL - 32, 1)
    low = iota((EXT, COL), 1) < 32
    both = jnp.where(low, both, 0.0)
    return both + pltpu.roll(both, 32, 1)


def piece_cols(s_ref, kx, ky):
    j = ((s_ref[2] - ky) & 3) * 4 + ((s_ref[3] - kx) & 3)
    return pl.ds(pl.multiple_of(j * COL, COL), COL)


def forward(where, t, cs, wg, wu, wd):
    d = TP * COL
    weight = pl.BlockSpec((1, HID, d), lambda i, s: (0, 0, 0))
    return pl.pallas_call(
        forward_kernel,
        grid_spec=pltpu.PrefetchScalarGridSpec(
            num_scalar_prefetch=1,
            grid=(BLK,),
            in_specs=[
                pl.BlockSpec((TP, NZ // BLK, 2 * CAP, COL), lambda i, s: (0, i, 0, 0)),
                *[pl.BlockSpec((4, NZ // BLK, 2 * CAP, COL), lambda i, s: (0, i, 0, 0))] * 4,
                weight,
                weight,
                weight,
            ],
            out_specs=[
                pl.BlockSpec((4, 1, RB + EXT, COL), lambda i, s: (0, i, 0, 0)),
                pl.BlockSpec((RB, HID), lambda i, s: (i, 0)),
            ],
            scratch_shapes=[
                pltpu.VMEM((RB, d), BF),
                pltpu.VMEM((RB, d), BF),
                pltpu.VMEM((2 * HID, d), BF),
                pltpu.VMEM((2 * HID, d), BF),
            ],
        ),
        out_shape=[
            jax.ShapeDtypeStruct((4, BLK, RB + EXT, COL), BF),
            jax.ShapeDtypeStruct((ROWS, HID), BF),
        ],
        name="forward",
        cost_estimate=pl.CostEstimate(flops=10**9, bytes_accessed=5 * 10**6, transcendentals=10**5),
    )(where, t, *cs, wg, wu, wd)


def back_kernel(s_ref, g_ref, w_ref, out_ref, w):
    @pl.when(pl.program_id(0) == 0)
    def _():
        for k in range(4):
            rows = pl.ds(pl.multiple_of(((s_ref[3] - k) & 3) * COL, COL), COL)
            for y in range(4):
                w[rows, y * COL : (y + 1) * COL] = w_ref[k, y]

    grads = jnp.concatenate([g_ref[x, 0, :RB] for x in range(4)], axis=1)
    pieces = dot(grads, w[...], 1, 0).astype(BF)
    parts = g_ref[0, 0, RB:].astype(F32)
    for x in range(1, 4):
        parts = parts + g_ref[x, 0, RB:].astype(F32)
    extra = two_parts(one_sum(parts))
    for y in range(4):
        out_ref[y, 0, :RB] = pieces[:, y * COL : (y + 1) * COL]
        out_ref[y, 0, RB:] = extra


def back(where, g, w):
    block = pl.BlockSpec((4, 1, RB + EXT, COL), lambda i, s: (0, i, 0, 0))
    return pl.pallas_call(
        back_kernel,
        grid_spec=pltpu.PrefetchScalarGridSpec(
            num_scalar_prefetch=1,
            grid=(BLK,),
            in_specs=[block, pl.BlockSpec((4, 4, 2 * HID, COL), lambda i, s: (0, 0, 0, 0))],
            out_specs=block,
            scratch_shapes=[pltpu.VMEM((4 * COL, 4 * COL), BF)],
        ),
        out_shape=jax.ShapeDtypeStruct((4, BLK, RB + EXT, COL), BF),
        compiler_params=pltpu.CompilerParams(vmem_limit_bytes=8 * 2**20),
        name="back",
        cost_estimate=pl.CostEstimate(flops=3 * 10**8, bytes_accessed=10**6, transcendentals=0),
    )(where, g, w)


def weights_kernel(s_ref, t_ref, c0_ref, c1_ref, c2_ref, c3_ref, g_ref, wt_ref, dg_ref, du_ref, dd_ref):
    grads = jnp.concatenate([g_ref[0, b, :RB] for b in range(BLK)], axis=0)
    for j in range(TP):
        cols = slice(j * COL, (j + 1) * COL)
        both = dot(grads, t_ref[j].reshape(ROWS, COL), 0, 0)
        dg_ref[0, :, cols] = both[:HID]
        du_ref[0, :, cols] = both[HID:]
    for kx, c_ref in enumerate((c0_ref, c1_ref, c2_ref, c3_ref)):
        for ky in range(4):
            dd_ref[0, :, piece_cols(s_ref, kx, ky)] = dot(
                wt_ref[...], c_ref[ky].reshape(ROWS, COL), 0, 0
            )


def weights(where, t, cs, g, wt):
    full = lambda *shape: pl.BlockSpec(shape, lambda i, s: (0,) * len(shape))
    d = TP * COL
    out = jax.ShapeDtypeStruct((1, HID, d), F32)
    return pl.pallas_call(
        weights_kernel,
        grid_spec=pltpu.PrefetchScalarGridSpec(
            num_scalar_prefetch=1,
            grid=(1,),
            in_specs=[
                full(TP, NZ, 2 * CAP, COL),
                *[full(4, NZ, 2 * CAP, COL)] * 4,
                full(1, BLK, RB + EXT, COL),
                full(ROWS, HID),
            ],
            out_specs=[full(1, HID, d)] * 3,
        ),
        out_shape=[out, out, out],
        name="weights",
        cost_estimate=pl.CostEstimate(flops=4 * 10**9, bytes_accessed=6 * 10**6, transcendentals=0),
    )(where, t, *cs, g, wt)


def total_kernel(p_ref, out_ref):
    rows = p_ref[0, 0].astype(F32)
    for y in range(1, 4):
        rows = rows + p_ref[y, 0].astype(F32)
    out_ref[:, : 2 * CAP] = rows[:RB].astype(BF).reshape(NZ // BLK, 2 * CAP, COL)
    extra = two_parts(one_sum(rows[RB:])).astype(F32)
    for k in range(NZ // BLK):
        out_ref[k, 2 * CAP :] = jnp.broadcast_to(extra[k : k + 1], (EXT, COL)).astype(BF)


def total(part):
    return pl.pallas_call(
        total_kernel,
        grid=(BLK,),
        in_specs=[pl.BlockSpec((4, 1, RB + EXT, COL), lambda i: (0, i, 0, 0))],
        out_specs=pl.BlockSpec((NZ // BLK, 2 * CAP + EXT, COL), lambda i: (i, 0, 0)),
        out_shape=jax.ShapeDtypeStruct((NZ, 2 * CAP + EXT, COL), BF),
        compiler_params=pltpu.CompilerParams(vmem_limit_bytes=4 * 2**20),
        name="total",
        cost_estimate=pl.CostEstimate(flops=10**7, bytes_accessed=2 * 10**6, transcendentals=0),
    )(part)


def combine_kernel(s_ref, ids_ref, w_ref, own_ref, other_ref, tok_ref, route_ref):
    core = s_ref[1]
    first, second, rank, _, chosen = routing(ids_ref, core)
    pick = jnp.where(chosen, 1.0, 0.0).astype(BF)
    half = NZ * CAP
    own = own_ref[:, :CAP].reshape(half, COL)
    other = other_ref[:, :CAP].reshape(half, COL)
    tok_ref[...] = (dot(pick[:half], own, 0, 0) + dot(pick[half:], other, 0, 0)).astype(BF)
    own_sums = own_ref[:, 2 * CAP :].reshape(NZ * EXT, COL)
    other_sums = other_ref[:, CAP:].reshape(NZ * EXT, COL)
    row = iota((NZ * EXT, TOK), 0)
    leads = (row & 7) == 0
    chip = row >> 3
    lane = iota((COL, TOK), 0)
    w = w_ref[...].astype(F32)
    for k, member in enumerate((first, second)):
        ids = ids_ref[k : k + 1, :]
        at = jnp.sum(member * rank, axis=0, keepdims=True).astype(I32)
        mine = (leads & (ids == 2 * chip + core)).astype(BF)
        theirs = (leads & (ids == 2 * chip + 1 - core)).astype(BF)
        near = dot(own_sums, mine, 0, 0)
        far = dot(other_sums, theirs, 0, 0)
        near = jnp.where((lane == at) | (lane == at + 32), near, 0.0)
        far = jnp.where((lane == at + 16) | (lane == at + 48), far, 0.0)
        route_ref[k : k + 1, :] = jnp.sum(near + far, axis=0, keepdims=True) / w[k : k + 1, :]


def combine(where, ids, w, own, other):
    full = lambda *shape: pl.BlockSpec(shape, lambda i, s: (0,) * len(shape))
    return pl.pallas_call(
        combine_kernel,
        grid_spec=pltpu.PrefetchScalarGridSpec(
            num_scalar_prefetch=1,
            grid=(1,),
            in_specs=[
                full(2, TOK),
                full(2, TOK),
                full(NZ, 2 * CAP + EXT, COL),
                full(NZ, CAP + EXT, COL),
            ],
            out_specs=[full(TOK, COL), full(2, TOK)],
        ),
        out_shape=[jax.ShapeDtypeStruct((TOK, COL), BF), jax.ShapeDtypeStruct((2, TOK), F32)],
        compiler_params=pltpu.CompilerParams(vmem_limit_bytes=4 * 2**20),
        name="combine",
        cost_estimate=pl.CostEstimate(flops=10**8, bytes_accessed=10**6, transcendentals=0),
    )(where, ids, w, own, other)


def exchange(x, axis):
    return lax.all_to_all(x, axis, split_axis=0, concat_axis=0, tiled=True)


def copies(x, n):
    return jnp.broadcast_to(x[None], (n, *x.shape))


def shifted(x, axis, by):
    n = lax.axis_size(axis)
    return lax.ppermute(x, axis, [(i, (i + by) % n) for i in range(n)])


def row_weights(gate_weight, up_weight, x):
    both = jnp.concatenate([gate_weight[0], up_weight[0]], axis=0)
    blocks = both.reshape(2 * HID, 4, 4, COL).transpose(2, 1, 0, 3)
    own = [lax.dynamic_index_in_dim(blocks, (x + k) & 3, 0, keepdims=False) for k in range(4)]
    moved = [shifted(own[k], "x", k) for k in range(1, 4)]
    return jnp.stack([own[0]] + moved)


def per_device(tokens, cotangent, expert_ids, route_weight, gate_weight, up_weight, down_weight):
    y, x, core = lax.axis_index("y"), lax.axis_index("x"), lax.axis_index("c")
    where = jnp.stack([y * 4 + x, core, y, x]).astype(I32)
    ids, w = expert_ids.T, route_weight.T
    own, other = dispatch(where, ids, w, tokens, cotangent)
    got = shifted(other, "c", 1)
    mine = jnp.stack([own, got], axis=2).reshape(NZ, 2, 2 * CAP, COL)
    mine = exchange(mine, "z")
    row_w = row_weights(gate_weight, up_weight, x)
    tok, cot = mine[:, 0], mine[:, 1]
    tok_row = exchange(copies(tok, 4), "x")
    cot_moved = [shifted(cot, "y", k) for k in range(1, 4)]
    cot_col = jnp.stack([cot] + cot_moved)
    tok_all = exchange(copies(tok_row, 4), "y").reshape(TP, NZ, 2 * CAP, COL)
    cot_all = [cot_col] + [shifted(cot_col, "x", k) for k in range(1, 4)]
    g, wt = forward(where, tok_all, cot_all, gate_weight, up_weight, down_weight)
    g_all = exchange(g, "x")
    part = back(where, g_all, row_w)
    sums = exchange(part, "y")
    gate_grad, up_grad, down_grad = weights(where, tok_all, cot_all, g, wt)
    home = exchange(total(sums), "z")
    far = shifted(home[:, CAP:], "c", 1)
    tokens_grad, route_grad = combine(where, ids, w, home, far)
    return tokens_grad, route_grad.T, gate_grad, up_grad, down_grad


def solution(mesh):
    grid = Mesh(mesh.devices.reshape(NZ, 2, 4, 4), ("z", "c", "y", "x"))
    ep, tp = ("z", "c"), ("y", "x")
    weight = P(ep, tp, None)
    return jax.shard_map(
        per_device,
        mesh=grid,
        in_specs=(P(ep, None), P(ep, None), P(ep, None), P(ep, None), weight, weight, weight),
        out_specs=(P(ep, tp), P(ep, None), weight, weight, weight),
        check_vma=False,
    )
```

```python
import jax
import jax.numpy as jnp
from jax import lax
from jax.experimental import pallas as pl
from jax.experimental.pallas import tpu as pltpu
from jax.sharding import Mesh
from jax.sharding import PartitionSpec as P


BF = jnp.bfloat16
F32 = jnp.float32
I32 = jnp.int32
NZ = 16
TP = 16
TOK = 128
CAP = 16
COL = 128
HID = 64
ROWS = 512
BLK = 4
RB = ROWS // BLK
SMALL = 12 * 2**20
EXT = 8


def iota(shape, dim):
    return lax.broadcasted_iota(I32, shape, dim)


def dot(a, b, ca, cb, precision=None):
    return lax.dot_general(
        a, b, (((ca,), (cb,)), ((), ())), precision=precision, preferred_element_type=F32
    )


def routing(ids_ref, core):
    experts = 2 * NZ
    row = iota((experts, TOK), 0)
    first = (ids_ref[0:1, :] == row).astype(F32)
    second = (ids_ref[1:2, :] == row).astype(F32)
    member = first + second
    earlier = (iota((TOK, TOK), 0) < iota((TOK, TOK), 1)).astype(BF)
    rank = dot(member.astype(BF), earlier, 1, 0)
    slots = 2 * NZ * CAP
    slot = iota((slots, experts), 0)
    half = slot >> 8
    expert = 2 * ((slot & 255) >> 4) + jnp.where(half == 0, core, 1 - core)
    expand = (expert == iota((slots, experts), 1)).astype(BF)
    hit = dot(expand, member.astype(BF), 1, 0)
    at = dot(expand, rank.astype(BF), 1, 0)
    place = (iota((slots, TOK), 0) & 15).astype(F32)
    chosen = (hit > 0.5) & (at == place)
    return first, second, rank, expand, chosen


def dispatch_kernel(s_ref, ids_ref, w_ref, tok_ref, cot_ref, own_ref, other_ref):
    first, second, _, expand, chosen = routing(ids_ref, s_ref[1])
    w = w_ref[...].astype(F32)
    weighted = first * w[0:1, :] + second * w[1:2, :]
    scale = dot(expand, weighted.astype(BF), 1, 0)
    pick = jnp.where(chosen, 1.0, 0.0).astype(BF)
    pick_scaled = jnp.where(chosen, scale, 0.0).astype(BF)
    rows = dot(pick, tok_ref[...], 1, 0).astype(BF)
    cots = dot(pick_scaled, cot_ref[...], 1, 0).astype(BF)
    half = NZ * CAP
    own_ref[:, 0] = rows[:half].reshape(NZ, CAP, COL)
    own_ref[:, 1] = cots[:half].reshape(NZ, CAP, COL)
    other_ref[:, 0] = rows[half:].reshape(NZ, CAP, COL)
    other_ref[:, 1] = cots[half:].reshape(NZ, CAP, COL)


def dispatch(where, ids, w, tokens, cotangent):
    full = lambda *shape: pl.BlockSpec(shape, lambda i, s: (0,) * len(shape))
    out = jax.ShapeDtypeStruct((NZ, 2, CAP, COL), BF)
    return pl.pallas_call(
        dispatch_kernel,
        grid_spec=pltpu.PrefetchScalarGridSpec(
            num_scalar_prefetch=1,
            grid=(1,),
            in_specs=[
                full(2, TOK),
                full(2, TOK),
                pl.BlockSpec((TOK, COL), lambda i, s: (0, s[0])),
                pl.BlockSpec((TOK, COL), lambda i, s: (0, s[0])),
            ],
            out_specs=[full(NZ, 2, CAP, COL)] * 2,
        ),
        out_shape=[out, out],
        name="dispatch",
        cost_estimate=pl.CostEstimate(flops=10**8, bytes_accessed=10**6, transcendentals=0),
    )(where, ids, w, tokens, cotangent)


def x_of(s_ref, k):
    return (s_ref[3] + k) & 3


def pack_kernel(s_ref, wg_ref, wu_ref, wd_ref, *out_refs):
    for k, out_ref in enumerate(out_refs):
        for y in range(4):
            cols = pl.ds(pl.multiple_of((y * 4 + x_of(s_ref, k)) * COL, COL), COL)
            out_ref[y, :HID] = wg_ref[0, :, cols]
            out_ref[y, HID : 2 * HID] = wu_ref[0, :, cols]
            out_ref[y, 2 * HID :] = wd_ref[0, :, cols]


def full(*shape):
    return pl.BlockSpec(shape, lambda i, s: (0,) * len(shape))


def call(kernel, where, args, in_specs, out_specs, out_shape, scratch=(), grid=1, flops=10**8, vmem=None):
    return pl.pallas_call(
        kernel,
        grid_spec=pltpu.PrefetchScalarGridSpec(
            num_scalar_prefetch=1,
            grid=(grid,),
            in_specs=in_specs,
            out_specs=out_specs,
            scratch_shapes=list(scratch),
        ),
        out_shape=out_shape,
        compiler_params=pltpu.CompilerParams(vmem_limit_bytes=vmem),
        cost_estimate=pl.CostEstimate(flops=flops, bytes_accessed=2 * 10**6, transcendentals=0),
    )(where, *args)


def pack(where, wg, wu, wd):
    shape = (4, 3 * HID, COL)
    return call(
        pack_kernel,
        where,
        (wg, wu, wd),
        [full(1, HID, TP * COL)] * 3,
        [full(*shape)] * 4,
        [jax.ShapeDtypeStruct(shape, BF)] * 4,
    )


def low_lanes(rows):
    return iota((rows, COL), 1) < HID


def features(x_ref, which, rows):
    return jnp.concatenate([x_ref[y, :, which].reshape(rows, COL) for y in range(4)], axis=1)


def pre_kernel(s_ref, x_ref, w_ref, out_ref, wgu, wdd):
    @pl.when(pl.program_id(0) == 0)
    def _():
        for k in range(4):
            for y in range(4):
                cols = slice(y * COL, (y + 1) * COL)
                wgu[k * COL : (k + 1) * COL, cols] = w_ref[k, y, : 2 * HID]
                wdd[k * COL : k * COL + HID, cols] = w_ref[k, y, 2 * HID :]
                wdd[k * COL + HID : (k + 1) * COL, cols] = w_ref[k, y, 2 * HID :]

    pre = dot(features(x_ref, 0, RB), wgu[...], 1, 1).astype(BF)
    back = dot(features(x_ref, 1, RB), wdd[...], 1, 1)
    for k in range(4):
        cols = slice(k * COL, (k + 1) * COL)
        to = x_of(s_ref, -k)
        half = back[:, cols]
        out_ref[to, 0, :RB] = pre[:, cols]
        out_ref[to, 0, RB:] = jnp.where(low_lanes(RB // 2), half[: RB // 2], half[RB // 2 :]).astype(BF)


PRE = RB + RB // 2
ACT = PRE + EXT


def pre_activations(where, x, w):
    return call(
        pre_kernel,
        where,
        (x, w),
        [
            pl.BlockSpec((4, NZ // BLK, 2, 2 * CAP, COL), lambda i, s: (0, i, 0, 0, 0)),
            full(4, 4, 3 * HID, COL),
        ],
        pl.BlockSpec((4, 1, PRE, COL), lambda i, s: (0, i, 0, 0)),
        jax.ShapeDtypeStruct((4, BLK, PRE, COL), BF),
        [pltpu.VMEM((4 * COL, 4 * COL), BF), pltpu.VMEM((4 * COL, 4 * COL), BF)],
        grid=BLK,
        vmem=SMALL,
    )


def act_kernel(s_ref, p_ref, g_ref):
    sums = p_ref[0, 0].astype(F32)
    for x in range(1, 4):
        sums = sums + p_ref[x, 0].astype(F32)
    pre, packed = sums[:RB], sums[RB:]
    low = low_lanes(RB // 2)
    other = pltpu.roll(packed, HID, 1)
    back = jnp.concatenate([jnp.where(low, packed, other), jnp.where(low, other, packed)], axis=0)
    lane = iota((RB, COL), 1)
    low_half = lane < HID
    turned = pltpu.roll(pre, HID, 1)
    gate = jnp.where(low_half, pre, turned)
    up = jnp.where(low_half, turned, pre)
    sigma = 1.0 / (1.0 + jnp.exp(-gate))
    silu = gate * sigma
    hidden = silu * up
    grads = jnp.where(low_half, back * up * sigma * (1.0 + gate * (1.0 - sigma)), back * silu).astype(BF)
    weighted = jnp.where(low, hidden[: RB // 2], hidden[RB // 2 :]).astype(BF)
    total = jnp.sum(jnp.where(low_half, hidden * back, 0.0), axis=1, keepdims=True)
    spread = jnp.where((lane & 31) == (iota((RB, COL), 0) & 31), total, 0.0)
    group = (iota((EXT, RB), 0) == (iota((EXT, RB), 1) >> 5)).astype(F32)
    extra = two_parts(dot(group, spread, 1, 0, lax.Precision.HIGHEST))
    for x in range(4):
        g_ref[x, 0, :RB] = grads
        g_ref[x, 0, RB:PRE] = weighted
        g_ref[x, 0, PRE:] = extra


def activations(where, p):
    return call(
        act_kernel,
        where,
        (p,),
        [pl.BlockSpec((4, 1, PRE, COL), lambda i, s: (0, i, 0, 0))],
        pl.BlockSpec((4, 1, ACT, COL), lambda i, s: (0, i, 0, 0)),
        jax.ShapeDtypeStruct((4, BLK, ACT, COL), BF),
        grid=BLK,
        vmem=SMALL,
    )


def two_parts(sums):
    high = sums.astype(BF).astype(F32)
    return jnp.where(iota((EXT, COL), 1) < 32, high, sums - high).astype(BF)


def one_sum(parts):
    both = parts + pltpu.roll(parts, COL - 32, 1)
    low = iota((EXT, COL), 1) < 32
    both = jnp.where(low, both, 0.0)
    return both + pltpu.roll(both, 32, 1)


def back_kernel(s_ref, g_ref, w_ref, out_ref, w):
    @pl.when(pl.program_id(0) == 0)
    def _():
        for k in range(4):
            rows = pl.ds(pl.multiple_of(x_of(s_ref, -k) * COL, COL), COL)
            for y in range(4):
                w[rows, y * COL : (y + 1) * COL] = w_ref[k, y, : 2 * HID]

    grads = jnp.concatenate([g_ref[x, 0, :RB] for x in range(4)], axis=1)
    pieces = dot(grads, w[...], 1, 0).astype(BF)
    parts = g_ref[0, 0, PRE:].astype(F32)
    for x in range(1, 4):
        parts = parts + g_ref[x, 0, PRE:].astype(F32)
    extra = two_parts(one_sum(parts))
    for y in range(4):
        out_ref[y, 0, :RB] = pieces[:, y * COL : (y + 1) * COL]
        out_ref[y, 0, RB:] = extra


def back(where, g, w):
    return call(
        back_kernel,
        where,
        (g, w),
        [pl.BlockSpec((4, 1, ACT, COL), lambda i, s: (0, i, 0, 0)), full(4, 4, 3 * HID, COL)],
        pl.BlockSpec((4, 1, RB + EXT, COL), lambda i, s: (0, i, 0, 0)),
        jax.ShapeDtypeStruct((4, BLK, RB + EXT, COL), BF),
        [pltpu.VMEM((4 * COL, 4 * COL), BF)],
        grid=BLK,
        vmem=SMALL,
    )


def weights_kernel(s_ref, x_ref, g_ref, own_ref, *out_refs):
    tok, cot = features(x_ref, 0, ROWS), features(x_ref, 1, ROWS)
    for k, out_ref in enumerate((own_ref, *out_refs)):
        owner = x_of(s_ref, k)
        grads = jnp.concatenate([g_ref[owner, b, :RB] for b in range(BLK)], axis=0)
        halves = []
        for b in range(BLK):
            packed = g_ref[owner, b, RB:PRE]
            halves += [packed, pltpu.roll(packed.astype(F32), HID, 1).astype(BF)]
        both = dot(grads, tok, 0, 0)
        down = dot(jnp.concatenate(halves, axis=0), cot, 0, 0)
        out_ref[: 2 * HID] = both.astype(out_ref.dtype)
        out_ref[2 * HID :] = down[:HID].astype(out_ref.dtype)


def weights(where, x, g):
    shape = (3 * HID, 4 * COL)
    return call(
        weights_kernel,
        where,
        (x, g),
        [full(4, NZ, 2, 2 * CAP, COL), full(4, BLK, ACT, COL)],
        [full(*shape)] * 4,
        [jax.ShapeDtypeStruct(shape, F32)] + [jax.ShapeDtypeStruct(shape, BF)] * 3,
        flops=4 * 10**9,
    )


def assemble_kernel(s_ref, *refs):
    *parts, dg_ref, du_ref, dd_ref = refs
    for k, p_ref in enumerate(parts):
        for y in range(4):
            cols = pl.ds(pl.multiple_of((y * 4 + x_of(s_ref, -k)) * COL, COL), COL)
            here = slice(y * COL, (y + 1) * COL)
            dg_ref[0, :, cols] = p_ref[:HID, here].astype(F32)
            du_ref[0, :, cols] = p_ref[HID : 2 * HID, here].astype(F32)
            dd_ref[0, :, cols] = p_ref[2 * HID :, here].astype(F32)


def assemble(where, parts):
    shape = (1, HID, TP * COL)
    return call(
        assemble_kernel,
        where,
        parts,
        [full(3 * HID, 4 * COL)] * 4,
        [full(*shape)] * 3,
        [jax.ShapeDtypeStruct(shape, F32)] * 3,
        flops=10**9,
    )


def total_kernel(p_ref, out_ref):
    rows = p_ref[0, 0].astype(F32)
    for y in range(1, 4):
        rows = rows + p_ref[y, 0].astype(F32)
    out_ref[:, : 2 * CAP] = rows[:RB].astype(BF).reshape(NZ // BLK, 2 * CAP, COL)
    extra = two_parts(one_sum(rows[RB:])).astype(F32)
    for k in range(NZ // BLK):
        out_ref[k, 2 * CAP :] = jnp.broadcast_to(extra[k : k + 1], (EXT, COL)).astype(BF)


def total(part):
    return pl.pallas_call(
        total_kernel,
        grid=(BLK,),
        in_specs=[pl.BlockSpec((4, 1, RB + EXT, COL), lambda i: (0, i, 0, 0))],
        out_specs=pl.BlockSpec((NZ // BLK, 2 * CAP + EXT, COL), lambda i: (i, 0, 0)),
        out_shape=jax.ShapeDtypeStruct((NZ, 2 * CAP + EXT, COL), BF),
        compiler_params=pltpu.CompilerParams(vmem_limit_bytes=4 * 2**20),
        name="total",
        cost_estimate=pl.CostEstimate(flops=10**7, bytes_accessed=2 * 10**6, transcendentals=0),
    )(part)


def combine_kernel(s_ref, ids_ref, w_ref, own_ref, other_ref, tok_ref, route_ref):
    core = s_ref[1]
    first, second, rank, _, chosen = routing(ids_ref, core)
    pick = jnp.where(chosen, 1.0, 0.0).astype(BF)
    half = NZ * CAP
    own = own_ref[:, :CAP].reshape(half, COL)
    other = other_ref[:, :CAP].reshape(half, COL)
    tok_ref[...] = (dot(pick[:half], own, 0, 0) + dot(pick[half:], other, 0, 0)).astype(BF)
    own_sums = own_ref[:, 2 * CAP :].reshape(NZ * EXT, COL)
    other_sums = other_ref[:, CAP:].reshape(NZ * EXT, COL)
    row = iota((NZ * EXT, TOK), 0)
    leads = (row & 7) == 0
    chip = row >> 3
    lane = iota((COL, TOK), 0)
    w = w_ref[...].astype(F32)
    for k, member in enumerate((first, second)):
        ids = ids_ref[k : k + 1, :]
        at = jnp.sum(member * rank, axis=0, keepdims=True).astype(I32)
        mine = (leads & (ids == 2 * chip + core)).astype(BF)
        theirs = (leads & (ids == 2 * chip + 1 - core)).astype(BF)
        near = dot(own_sums, mine, 0, 0)
        far = dot(other_sums, theirs, 0, 0)
        near = jnp.where((lane == at) | (lane == at + 32), near, 0.0)
        far = jnp.where((lane == at + 16) | (lane == at + 48), far, 0.0)
        route_ref[k : k + 1, :] = jnp.sum(near + far, axis=0, keepdims=True) / w[k : k + 1, :]


def combine(where, ids, w, own, other):
    full = lambda *shape: pl.BlockSpec(shape, lambda i, s: (0,) * len(shape))
    return pl.pallas_call(
        combine_kernel,
        grid_spec=pltpu.PrefetchScalarGridSpec(
            num_scalar_prefetch=1,
            grid=(1,),
            in_specs=[
                full(2, TOK),
                full(2, TOK),
                full(NZ, 2 * CAP + EXT, COL),
                full(NZ, CAP + EXT, COL),
            ],
            out_specs=[full(TOK, COL), full(2, TOK)],
        ),
        out_shape=[jax.ShapeDtypeStruct((TOK, COL), BF), jax.ShapeDtypeStruct((2, TOK), F32)],
        compiler_params=pltpu.CompilerParams(vmem_limit_bytes=4 * 2**20),
        name="combine",
        cost_estimate=pl.CostEstimate(flops=10**8, bytes_accessed=10**6, transcendentals=0),
    )(where, ids, w, own, other)


def exchange(x, axis):
    return lax.all_to_all(x, axis, split_axis=0, concat_axis=0, tiled=True)


def copies(x, n):
    return jnp.broadcast_to(x[None], (n, *x.shape))


def shifted(x, axis, by):
    n = lax.axis_size(axis)
    return lax.ppermute(x, axis, [(i, (i + by) % n) for i in range(n)])


def row_weights(where, wg, wu, wd):
    own, *others = pack(where, wg, wu, wd)
    moved = [shifted(other, "x", k + 1) for k, other in enumerate(others)]
    return jnp.stack([own, *moved])


def per_device(tokens, cotangent, expert_ids, route_weight, gate_weight, up_weight, down_weight):
    y, x, core = lax.axis_index("y"), lax.axis_index("x"), lax.axis_index("c")
    where = jnp.stack([y * 4 + x, core, y, x]).astype(I32)
    ids, w = expert_ids.T, route_weight.T
    own, other = dispatch(where, ids, w, tokens, cotangent)
    got = shifted(other, "c", 1)
    mine = jnp.stack([own, got], axis=2).reshape(NZ, 2, 2 * CAP, COL)
    mine = exchange(mine, "z")
    row_w = row_weights(where, gate_weight, up_weight, down_weight)
    rows = exchange(copies(mine, 4), "y")
    pre = pre_activations(where, rows, row_w)
    pre = exchange(pre, "x")
    g = activations(where, pre)
    g = exchange(g, "x")
    part = back(where, g, row_w)
    sums = exchange(part, "y")
    kept, *sent = weights(where, rows, g)
    home = exchange(total(sums), "z")
    moved = [shifted(part, "x", k + 1) for k, part in enumerate(sent)]
    gate_grad, up_grad, down_grad = assemble(where, (kept, *moved))
    far = shifted(home[:, CAP:], "c", 1)
    tokens_grad, route_grad = combine(where, ids, w, home, far)
    return tokens_grad, route_grad.T, gate_grad, up_grad, down_grad


def solution(mesh):
    grid = Mesh(mesh.devices.reshape(NZ, 2, 4, 4), ("z", "c", "y", "x"))
    ep, tp = ("z", "c"), ("y", "x")
    weight = P(ep, tp, None)
    return jax.shard_map(
        per_device,
        mesh=grid,
        in_specs=(P(ep, None), P(ep, None), P(ep, None), P(ep, None), weight, weight, weight),
        out_specs=(P(ep, tp), P(ep, None), weight, weight, weight),
        check_vma=False,
    )
```

```python
import jax
import jax.numpy as jnp
from jax import lax
from jax.experimental import pallas as pl
from jax.experimental.pallas import tpu as pltpu
from jax.sharding import Mesh
from jax.sharding import PartitionSpec as P


BF = jnp.bfloat16
F32 = jnp.float32
I32 = jnp.int32
NZ = 16
TP = 16
TOK = 128
CAP = 16
COL = 128
HID = 64
ROWS = 512
BLK = 4
RB = ROWS // BLK
SMALL = 12 * 2**20
EXT = 8


def iota(shape, dim):
    return lax.broadcasted_iota(I32, shape, dim)


def dot(a, b, ca, cb, precision=None):
    return lax.dot_general(
        a, b, (((ca,), (cb,)), ((), ())), precision=precision, preferred_element_type=F32
    )


def routing(ids_ref):
    experts = 2 * NZ
    row = iota((experts, TOK), 0)
    first = (ids_ref[0:1, :] == row).astype(F32)
    second = (ids_ref[1:2, :] == row).astype(F32)
    member = first + second
    earlier = (iota((TOK, TOK), 0) < iota((TOK, TOK), 1)).astype(BF)
    rank = dot(member.astype(BF), earlier, 1, 0)
    slots = experts * CAP
    expand = ((iota((slots, experts), 0) >> 4) == iota((slots, experts), 1)).astype(BF)
    hit = dot(expand, member.astype(BF), 1, 0)
    at = dot(expand, rank.astype(BF), 1, 0)
    place = (iota((slots, TOK), 0) & 15).astype(F32)
    chosen = (hit > 0.5) & (at == place)
    return first, second, rank, expand, chosen


def dispatch_kernel(s_ref, ids_ref, w_ref, tok_ref, cot_ref, out_ref):
    first, second, _, expand, chosen = routing(ids_ref)
    w = w_ref[...].astype(F32)
    weighted = first * w[0:1, :] + second * w[1:2, :]
    scale = dot(expand, weighted.astype(BF), 1, 0)
    pick = jnp.where(chosen, 1.0, 0.0).astype(BF)
    pick_scaled = jnp.where(chosen, scale, 0.0).astype(BF)
    out_ref[:, :, 0] = dot(pick, tok_ref[...], 1, 0).astype(BF).reshape(NZ, 2, CAP, COL)
    out_ref[:, :, 1] = dot(pick_scaled, cot_ref[...], 1, 0).astype(BF).reshape(NZ, 2, CAP, COL)


def dispatch(where, ids, w, tokens, cotangent):
    mine = pl.BlockSpec((TOK, COL), lambda i, s: (0, s[0]))
    return call(
        dispatch_kernel,
        where,
        (ids, w, tokens, cotangent),
        [full(2, TOK), full(2, TOK), mine, mine],
        full(NZ, 2, 2, CAP, COL),
        jax.ShapeDtypeStruct((NZ, 2, 2, CAP, COL), BF),
    )


def x_of(s_ref, k):
    return (s_ref[1] + k) & 3


def pack_kernel(s_ref, wg_ref, wu_ref, wd_ref, *out_refs):
    for k, out_ref in enumerate(out_refs):
        for y in range(4):
            cols = pl.ds(pl.multiple_of((y * 4 + x_of(s_ref, k)) * COL, COL), COL)
            out_ref[y, :HID] = wg_ref[0, :, cols]
            out_ref[y, HID : 2 * HID] = wu_ref[0, :, cols]
            out_ref[y, 2 * HID :] = wd_ref[0, :, cols]


def full(*shape):
    return pl.BlockSpec(shape, lambda i, s: (0,) * len(shape))


def call(kernel, where, args, in_specs, out_specs, out_shape, scratch=(), grid=1, flops=10**8, vmem=None):
    return pl.pallas_call(
        kernel,
        grid_spec=pltpu.PrefetchScalarGridSpec(
            num_scalar_prefetch=1,
            grid=(grid,),
            in_specs=in_specs,
            out_specs=out_specs,
            scratch_shapes=list(scratch),
        ),
        out_shape=out_shape,
        compiler_params=pltpu.CompilerParams(vmem_limit_bytes=vmem),
        cost_estimate=pl.CostEstimate(flops=flops, bytes_accessed=2 * 10**6, transcendentals=0),
    )(where, *args)


def pack(where, wg, wu, wd):
    shape = (4, 3 * HID, COL)
    return call(
        pack_kernel,
        where,
        (wg, wu, wd),
        [full(1, HID, TP * COL)] * 3,
        [full(*shape)] * 4,
        [jax.ShapeDtypeStruct(shape, BF)] * 4,
    )


def low_lanes(rows):
    return iota((rows, COL), 1) < HID


def features(x_ref, which, rows):
    return jnp.concatenate([x_ref[:, y, :, which].reshape(rows, COL) for y in range(4)], axis=1)


def pre_kernel(s_ref, x_ref, w_ref, out_ref, wgu, wdd):
    @pl.when(pl.program_id(0) == 0)
    def _():
        for k in range(4):
            for y in range(4):
                cols = slice(y * COL, (y + 1) * COL)
                wgu[k * COL : (k + 1) * COL, cols] = w_ref[k, y, : 2 * HID]
                wdd[k * COL : k * COL + HID, cols] = w_ref[k, y, 2 * HID :]
                wdd[k * COL + HID : (k + 1) * COL, cols] = w_ref[k, y, 2 * HID :]

    pre = dot(features(x_ref, 0, RB), wgu[...], 1, 1).astype(BF)
    back = dot(features(x_ref, 1, RB), wdd[...], 1, 1)
    for k in range(4):
        cols = slice(k * COL, (k + 1) * COL)
        to = x_of(s_ref, -k)
        half = back[:, cols]
        out_ref[to, 0, :RB] = pre[:, cols]
        out_ref[to, 0, RB:] = jnp.where(low_lanes(RB // 2), half[: RB // 2], half[RB // 2 :]).astype(BF)


PRE = RB + RB // 2
ACT = PRE + EXT
HOME = RB // 2 + EXT


def pre_activations(where, x, w):
    return call(
        pre_kernel,
        where,
        (x, w),
        [
            pl.BlockSpec((2, 4, NZ // BLK, 2, CAP, COL), lambda i, s: (0, 0, i, 0, 0, 0)),
            full(4, 4, 3 * HID, COL),
        ],
        pl.BlockSpec((4, 1, PRE, COL), lambda i, s: (0, i, 0, 0)),
        jax.ShapeDtypeStruct((4, BLK, PRE, COL), BF),
        [pltpu.VMEM((4 * COL, 4 * COL), BF), pltpu.VMEM((4 * COL, 4 * COL), BF)],
        grid=BLK,
        vmem=SMALL,
    )


def act_kernel(s_ref, p_ref, g_ref):
    sums = p_ref[0, 0].astype(F32)
    for x in range(1, 4):
        sums = sums + p_ref[x, 0].astype(F32)
    pre, packed = sums[:RB], sums[RB:]
    low = low_lanes(RB // 2)
    other = pltpu.roll(packed, HID, 1)
    back = jnp.concatenate([jnp.where(low, packed, other), jnp.where(low, other, packed)], axis=0)
    lane = iota((RB, COL), 1)
    low_half = lane < HID
    turned = pltpu.roll(pre, HID, 1)
    gate = jnp.where(low_half, pre, turned)
    up = jnp.where(low_half, turned, pre)
    sigma = 1.0 / (1.0 + jnp.exp(-gate))
    silu = gate * sigma
    hidden = silu * up
    grads = jnp.where(low_half, back * up * sigma * (1.0 + gate * (1.0 - sigma)), back * silu).astype(BF)
    weighted = jnp.where(low, hidden[: RB // 2], hidden[RB // 2 :]).astype(BF)
    total = jnp.sum(jnp.where(low_half, hidden * back, 0.0), axis=1, keepdims=True)
    spread = jnp.where((lane & 15) == (iota((RB, COL), 0) & 15), total, 0.0)
    group = (iota((EXT, RB), 0) == (iota((EXT, RB), 1) >> 4)).astype(F32)
    extra = two_parts(dot(group, spread, 1, 0, lax.Precision.HIGHEST))
    for x in range(4):
        g_ref[x, 0, :RB] = grads
        g_ref[x, 0, RB:PRE] = weighted
        g_ref[x, 0, PRE:] = extra


def activations(where, p):
    return call(
        act_kernel,
        where,
        (p,),
        [pl.BlockSpec((4, 1, PRE, COL), lambda i, s: (0, i, 0, 0))],
        pl.BlockSpec((4, 1, ACT, COL), lambda i, s: (0, i, 0, 0)),
        jax.ShapeDtypeStruct((4, BLK, ACT, COL), BF),
        grid=BLK,
        vmem=SMALL,
    )


def two_parts(sums):
    high = sums.astype(BF).astype(F32)
    return jnp.where(iota((EXT, COL), 1) < 32, high, sums - high).astype(BF)


def one_sum(parts):
    both = parts + pltpu.roll(parts, COL - 32, 1)
    low = iota((EXT, COL), 1) < 32
    both = jnp.where(low, both, 0.0)
    return both + pltpu.roll(both, 32, 1)


def back_kernel(s_ref, g_ref, w_ref, out_ref, w):
    @pl.when(pl.program_id(0) == 0)
    def _():
        for k in range(4):
            rows = pl.ds(pl.multiple_of(x_of(s_ref, -k) * COL, COL), COL)
            for y in range(4):
                w[rows, y * COL : (y + 1) * COL] = w_ref[k, y, : 2 * HID]

    grads = jnp.concatenate([g_ref[x, 0, :RB] for x in range(4)], axis=1)
    pieces = dot(grads, w[...], 1, 0).astype(BF)
    parts = g_ref[0, 0, PRE:].astype(F32)
    for x in range(1, 4):
        parts = parts + g_ref[x, 0, PRE:].astype(F32)
    sums = one_sum(parts)
    half = RB // 2
    for core in range(2):
        extra = two_parts(sums if core == 0 else pltpu.roll(sums, EXT // 2, 0))
        for y in range(4):
            out_ref[core, y, 0, :half] = pieces[core * half : (core + 1) * half, y * COL : (y + 1) * COL]
            out_ref[core, y, 0, half:] = extra


def back(where, g, w):
    return call(
        back_kernel,
        where,
        (g, w),
        [pl.BlockSpec((4, 1, ACT, COL), lambda i, s: (0, i, 0, 0)), full(4, 4, 3 * HID, COL)],
        pl.BlockSpec((2, 4, 1, HOME, COL), lambda i, s: (0, 0, i, 0, 0)),
        jax.ShapeDtypeStruct((2, 4, BLK, HOME, COL), BF),
        [pltpu.VMEM((4 * COL, 4 * COL), BF)],
        grid=BLK,
        vmem=SMALL,
    )


def weights_kernel(s_ref, x_ref, g_ref, own_ref, *out_refs):
    near = NZ // BLK
    blocks = [x_ref.at[:, :, b * near : (b + 1) * near] for b in range(BLK)]
    tok, cot = (jnp.concatenate([features(b, which, RB) for b in blocks], axis=0) for which in range(2))
    for k, out_ref in enumerate((own_ref, *out_refs)):
        owner = x_of(s_ref, k)
        grads = jnp.concatenate([g_ref[owner, b, :RB] for b in range(BLK)], axis=0)
        halves = []
        for b in range(BLK):
            packed = g_ref[owner, b, RB:PRE]
            halves += [packed, pltpu.roll(packed.astype(F32), HID, 1).astype(BF)]
        both = dot(grads, tok, 0, 0)
        down = dot(jnp.concatenate(halves, axis=0), cot, 0, 0)
        out_ref[: 2 * HID] = both.astype(out_ref.dtype)
        out_ref[2 * HID :] = down[:HID].astype(out_ref.dtype)


def weights(where, x, g):
    shape = (3 * HID, 4 * COL)
    return call(
        weights_kernel,
        where,
        (x, g),
        [full(2, 4, NZ, 2, CAP, COL), full(4, BLK, ACT, COL)],
        [full(*shape)] * 4,
        [jax.ShapeDtypeStruct(shape, F32)] + [jax.ShapeDtypeStruct(shape, BF)] * 3,
        flops=4 * 10**9,
    )


def assemble_kernel(s_ref, *refs):
    *parts, dg_ref, du_ref, dd_ref = refs
    for k, p_ref in enumerate(parts):
        for y in range(4):
            cols = pl.ds(pl.multiple_of((y * 4 + x_of(s_ref, -k)) * COL, COL), COL)
            here = slice(y * COL, (y + 1) * COL)
            dg_ref[0, :, cols] = p_ref[:HID, here].astype(F32)
            du_ref[0, :, cols] = p_ref[HID : 2 * HID, here].astype(F32)
            dd_ref[0, :, cols] = p_ref[2 * HID :, here].astype(F32)


def assemble(where, parts):
    shape = (1, HID, TP * COL)
    return call(
        assemble_kernel,
        where,
        parts,
        [full(3 * HID, 4 * COL)] * 4,
        [full(*shape)] * 3,
        [jax.ShapeDtypeStruct(shape, F32)] * 3,
        flops=10**9,
    )


def total_kernel(s_ref, p_ref, out_ref):
    half, sums = RB // 2, []
    for core in range(2):
        rows = p_ref[core, 0, 0].astype(F32)
        for y in range(1, 4):
            rows = rows + p_ref[core, y, 0].astype(F32)
        out_ref[:, core * CAP : (core + 1) * CAP] = rows[:half].astype(BF).reshape(NZ // BLK, CAP, COL)
        sums.append(one_sum(rows[half:]))
    extra = two_parts(jnp.where((iota((EXT, COL), 1) & 31) < 16, *sums)).astype(F32)
    for k in range(NZ // BLK):
        out_ref[k, 2 * CAP :] = jnp.broadcast_to(extra[k : k + 1], (EXT, COL)).astype(BF)


def total(where, part):
    return call(
        total_kernel,
        where,
        (part,),
        [pl.BlockSpec((2, 4, 1, HOME, COL), lambda i, s: (0, 0, i, 0, 0))],
        pl.BlockSpec((NZ // BLK, 2 * CAP + EXT, COL), lambda i, s: (i, 0, 0)),
        jax.ShapeDtypeStruct((NZ, 2 * CAP + EXT, COL), BF),
        grid=BLK,
        vmem=4 * 2**20,
    )


def combine_kernel(s_ref, ids_ref, w_ref, home_ref, tok_ref, route_ref):
    first, second, rank, _, chosen = routing(ids_ref)
    pick = jnp.where(chosen, 1.0, 0.0).astype(BF)
    rows = home_ref[:, : 2 * CAP].reshape(2 * NZ * CAP, COL)
    tok_ref[...] = dot(pick, rows, 0, 0).astype(BF)
    sums = home_ref[:, 2 * CAP :].reshape(NZ * EXT, COL)
    row = iota((NZ * EXT, TOK), 0)
    lane = iota((COL, TOK), 0)
    w = w_ref[...].astype(F32)
    for k, member in enumerate((first, second)):
        ids = ids_ref[k : k + 1, :]
        at = jnp.sum(member * rank, axis=0, keepdims=True).astype(I32) + 16 * (ids & 1)
        chip = (((row & 7) == 0) & ((row >> 3) == (ids >> 1))).astype(BF)
        found = dot(sums, chip, 0, 0)
        found = jnp.where((lane == at) | (lane == at + 32), found, 0.0)
        route_ref[k : k + 1, :] = jnp.sum(found, axis=0, keepdims=True) / w[k : k + 1, :]


def combine(where, ids, w, home):
    return call(
        combine_kernel,
        where,
        (ids, w, home),
        [full(2, TOK), full(2, TOK), full(NZ, 2 * CAP + EXT, COL)],
        [full(TOK, COL), full(2, TOK)],
        [jax.ShapeDtypeStruct((TOK, COL), BF), jax.ShapeDtypeStruct((2, TOK), F32)],
        vmem=4 * 2**20,
    )


def exchange(x, axis):
    return lax.all_to_all(x, axis, split_axis=0, concat_axis=0, tiled=True)


def copies(x, n):
    return jnp.broadcast_to(x[None], (n, *x.shape))


def shifted(x, axis, by):
    n = lax.axis_size(axis)
    return lax.ppermute(x, axis, [(i, (i + by) % n) for i in range(n)])


def row_weights(where, wg, wu, wd):
    own, *others = pack(where, wg, wu, wd)
    moved = [shifted(other, "x", k + 1) for k, other in enumerate(others)]
    return jnp.stack([own, *moved])


def per_device(tokens, cotangent, expert_ids, route_weight, gate_weight, up_weight, down_weight):
    y, x = lax.axis_index("y"), lax.axis_index("x")
    where = jnp.stack([y * 4 + x, x]).astype(I32)
    ids, w = expert_ids.T, route_weight.T
    mine = exchange(dispatch(where, ids, w, tokens, cotangent), "z")
    row_w = row_weights(where, gate_weight, up_weight, down_weight)
    both = copies(mine.transpose(1, 0, 2, 3, 4), 4).transpose(1, 0, 2, 3, 4, 5)
    rows = exchange(both.reshape(8, NZ, 2, CAP, COL), ("c", "y")).reshape(both.shape)
    pre = pre_activations(where, rows, row_w)
    pre = exchange(pre, "x")
    g = activations(where, pre)
    g = exchange(g, "x")
    part = back(where, g, row_w)
    sums = exchange(part.reshape(8, BLK, HOME, COL), ("c", "y")).reshape(part.shape)
    kept, *sent = weights(where, rows, g)
    home = exchange(total(where, sums), "z")
    moved = [shifted(part, "x", k + 1) for k, part in enumerate(sent)]
    gate_grad, up_grad, down_grad = assemble(where, (kept, *moved))
    tokens_grad, route_grad = combine(where, ids, w, home)
    return tokens_grad, route_grad.T, gate_grad, up_grad, down_grad


def solution(mesh):
    grid = Mesh(mesh.devices.reshape(NZ, 2, 4, 4), ("z", "c", "y", "x"))
    ep, tp = ("z", "c"), ("y", "x")
    weight = P(ep, tp, None)
    return jax.shard_map(
        per_device,
        mesh=grid,
        in_specs=(P(ep, None), P(ep, None), P(ep, None), P(ep, None), weight, weight, weight),
        out_specs=(P(ep, tp), P(ep, None), weight, weight, weight),
        check_vma=False,
    )
```

```python
import jax
import jax.numpy as jnp
from jax import lax
from jax.experimental import pallas as pl
from jax.experimental.pallas import tpu as pltpu
from jax.sharding import Mesh
from jax.sharding import PartitionSpec as P


BF = jnp.bfloat16
F32 = jnp.float32
I32 = jnp.int32
NZ = 16
TP = 16
TOK = 128
CAP = 16
COL = 128
HID = 64
ROWS = 512
BLK = 2
RB = ROWS // BLK
SMALL = 12 * 2**20
EXT = 2 * NZ // BLK
DUP = 8


def iota(shape, dim):
    return lax.broadcasted_iota(I32, shape, dim)


def dot(a, b, ca, cb, precision=None):
    return lax.dot_general(
        a, b, (((ca,), (cb,)), ((), ())), precision=precision, preferred_element_type=F32
    )


def routing(ids_ref):
    experts = 2 * NZ
    row = iota((experts, TOK), 0)
    first = (ids_ref[0:1, :] == row).astype(F32)
    second = (ids_ref[1:2, :] == row).astype(F32)
    member = first + second
    earlier = (iota((TOK, TOK), 0) < iota((TOK, TOK), 1)).astype(BF)
    rank = dot(member.astype(BF), earlier, 1, 0)
    slots = experts * CAP
    expand = ((iota((slots, experts), 0) >> 4) == iota((slots, experts), 1)).astype(BF)
    hit = dot(expand, member.astype(BF), 1, 0)
    at = dot(expand, rank.astype(BF), 1, 0)
    place = (iota((slots, TOK), 0) & 15).astype(F32)
    chosen = (hit > 0.5) & (at == place)
    return first, second, rank, expand, chosen


def dispatch_kernel(s_ref, ids_ref, w_ref, tok_ref, cot_ref, out_ref):
    first, second, _, expand, chosen = routing(ids_ref)
    w = w_ref[...].astype(F32)
    weighted = first * w[0:1, :] + second * w[1:2, :]
    scale = dot(expand, weighted.astype(BF), 1, 0)
    pick = jnp.where(chosen, 1.0, 0.0).astype(BF)
    pick_scaled = jnp.where(chosen, scale, 0.0).astype(BF)
    out_ref[:, :, 0] = dot(pick, tok_ref[...], 1, 0).astype(BF).reshape(NZ, 2, CAP, COL)
    out_ref[:, :, 1] = dot(pick_scaled, cot_ref[...], 1, 0).astype(BF).reshape(NZ, 2, CAP, COL)


def dispatch(where, ids, w, tokens, cotangent):
    mine = pl.BlockSpec((TOK, COL), lambda i, s: (0, s[0]))
    return call(
        dispatch_kernel,
        where,
        (ids, w, tokens, cotangent),
        [full(2, TOK), full(2, TOK), mine, mine],
        full(NZ, 2, 2, CAP, COL),
        jax.ShapeDtypeStruct((NZ, 2, 2, CAP, COL), BF),
    )


def x_of(s_ref, k):
    return (s_ref[1] + k) & 3


def pack_kernel(s_ref, wg_ref, wu_ref, wd_ref, *out_refs):
    for k, out_ref in enumerate(out_refs):
        for y in range(4):
            cols = pl.ds(pl.multiple_of((y * 4 + x_of(s_ref, k)) * COL, COL), COL)
            out_ref[y, :HID] = wg_ref[0, :, cols]
            out_ref[y, HID : 2 * HID] = wu_ref[0, :, cols]
            out_ref[y, 2 * HID :] = wd_ref[0, :, cols]


def full(*shape):
    return pl.BlockSpec(shape, lambda i, s: (0,) * len(shape))


def call(kernel, where, args, in_specs, out_specs, out_shape, scratch=(), grid=1, flops=10**8, vmem=None):
    return pl.pallas_call(
        kernel,
        grid_spec=pltpu.PrefetchScalarGridSpec(
            num_scalar_prefetch=1,
            grid=(grid,),
            in_specs=in_specs,
            out_specs=out_specs,
            scratch_shapes=list(scratch),
        ),
        out_shape=out_shape,
        compiler_params=pltpu.CompilerParams(vmem_limit_bytes=vmem),
        cost_estimate=pl.CostEstimate(flops=flops, bytes_accessed=2 * 10**6, transcendentals=0),
    )(where, *args)


def pack(where, wg, wu, wd):
    shape = (4, 3 * HID, COL)
    return call(
        pack_kernel,
        where,
        (wg, wu, wd),
        [full(1, HID, TP * COL)] * 3,
        [full(*shape)] * 4,
        [jax.ShapeDtypeStruct(shape, BF)] * 4,
    )


def low_lanes(rows):
    return iota((rows, COL), 1) < HID


def features(x_ref, which, rows):
    return jnp.concatenate([x_ref[:, y, :, which].reshape(rows, COL) for y in range(4)], axis=1)


def layout_kernel(s_ref, w0_ref, w1_ref, w2_ref, w3_ref, wgu_ref, wdd_ref):
    for k, w_ref in enumerate((w0_ref, w1_ref, w2_ref, w3_ref)):
        for y in range(4):
            cols = slice(y * COL, (y + 1) * COL)
            wgu_ref[k * COL : (k + 1) * COL, cols] = w_ref[y, : 2 * HID]
            wdd_ref[k * COL : k * COL + HID, cols] = w_ref[y, 2 * HID :]
            wdd_ref[k * COL + HID : (k + 1) * COL, cols] = w_ref[y, 2 * HID :]


def layout(where, ws):
    shape = (4 * COL, 4 * COL)
    return call(
        layout_kernel,
        where,
        ws,
        [full(4, 3 * HID, COL)] * 4,
        [full(*shape)] * 2,
        [jax.ShapeDtypeStruct(shape, BF)] * 2,
        vmem=SMALL,
    )


def pre_kernel(s_ref, x_ref, wgu_ref, wdd_ref, out_ref):
    pre = dot(features(x_ref, 0, RB), wgu_ref[...], 1, 1).astype(BF)
    back = dot(features(x_ref, 1, RB), wdd_ref[...], 1, 1)
    for k in range(4):
        cols = slice(k * COL, (k + 1) * COL)
        to = x_of(s_ref, -k)
        half = back[:, cols]
        out_ref[to, 0, :RB] = pre[:, cols]
        out_ref[to, 0, RB:] = jnp.where(low_lanes(RB // 2), half[: RB // 2], half[RB // 2 :]).astype(BF)


PRE = RB + RB // 2
ACT = PRE + EXT
HOME = RB // 2 + EXT


def pre_activations(where, x, wgu, wdd):
    return call(
        pre_kernel,
        where,
        (x, wgu, wdd),
        [
            pl.BlockSpec((2, 4, NZ // BLK, 2, CAP, COL), lambda i, s: (0, 0, i, 0, 0, 0)),
            full(4 * COL, 4 * COL),
            full(4 * COL, 4 * COL),
        ],
        pl.BlockSpec((4, 1, PRE, COL), lambda i, s: (0, i, 0, 0)),
        jax.ShapeDtypeStruct((4, BLK, PRE, COL), BF),
        grid=BLK,
        vmem=SMALL,
    )


def act_kernel(s_ref, p_ref, g_ref):
    sums = p_ref[0, 0].astype(F32)
    for x in range(1, 4):
        sums = sums + p_ref[x, 0].astype(F32)
    pre, packed = sums[:RB], sums[RB:]
    low = low_lanes(RB // 2)
    other = pltpu.roll(packed, HID, 1)
    back = jnp.concatenate([jnp.where(low, packed, other), jnp.where(low, other, packed)], axis=0)
    lane = iota((RB, COL), 1)
    low_half = lane < HID
    turned = pltpu.roll(pre, HID, 1)
    gate = jnp.where(low_half, pre, turned)
    up = jnp.where(low_half, turned, pre)
    sigma = 1.0 / (1.0 + jnp.exp(-gate))
    silu = gate * sigma
    hidden = silu * up
    grads = jnp.where(low_half, back * up * sigma * (1.0 + gate * (1.0 - sigma)), back * silu).astype(BF)
    weighted = jnp.where(low, hidden[: RB // 2], hidden[RB // 2 :]).astype(BF)
    total = jnp.sum(jnp.where(low_half, hidden * back, 0.0), axis=1, keepdims=True)
    spread = jnp.where((lane & 15) == (iota((RB, COL), 0) & 15), total, 0.0)
    group = (iota((EXT, RB), 0) == (iota((EXT, RB), 1) >> 4)).astype(F32)
    extra = two_parts(dot(group, spread, 1, 0, lax.Precision.HIGHEST))
    for x in range(4):
        g_ref[x, 0, :RB] = grads
        g_ref[x, 0, RB:PRE] = weighted
        g_ref[x, 0, PRE:] = extra


def activations(where, p):
    return call(
        act_kernel,
        where,
        (p,),
        [pl.BlockSpec((4, 1, PRE, COL), lambda i, s: (0, i, 0, 0))],
        pl.BlockSpec((4, 1, ACT, COL), lambda i, s: (0, i, 0, 0)),
        jax.ShapeDtypeStruct((4, BLK, ACT, COL), BF),
        grid=BLK,
        vmem=SMALL,
    )


def two_parts(sums):
    high = sums.astype(BF).astype(F32)
    return jnp.where(iota((EXT, COL), 1) < 32, high, sums - high).astype(BF)


def one_sum(parts):
    both = parts + pltpu.roll(parts, COL - 32, 1)
    low = iota((EXT, COL), 1) < 32
    both = jnp.where(low, both, 0.0)
    return both + pltpu.roll(both, 32, 1)


def back_kernel(s_ref, g_ref, w_ref, out_ref):
    grads = jnp.concatenate([g_ref[x_of(s_ref, -k), 0, :RB] for k in range(4)], axis=1)
    pieces = dot(grads, w_ref[...], 1, 0).astype(BF)
    parts = g_ref[0, 0, PRE:].astype(F32)
    for x in range(1, 4):
        parts = parts + g_ref[x, 0, PRE:].astype(F32)
    sums = one_sum(parts)
    half = RB // 2
    for core in range(2):
        extra = two_parts(sums if core == 0 else pltpu.roll(sums, EXT // 2, 0))
        for y in range(4):
            out_ref[core, y, 0, :half] = pieces[core * half : (core + 1) * half, y * COL : (y + 1) * COL]
            out_ref[core, y, 0, half:] = extra


def back(where, g, w):
    return call(
        back_kernel,
        where,
        (g, w),
        [pl.BlockSpec((4, 1, ACT, COL), lambda i, s: (0, i, 0, 0)), full(4 * COL, 4 * COL)],
        pl.BlockSpec((2, 4, 1, HOME, COL), lambda i, s: (0, 0, i, 0, 0)),
        jax.ShapeDtypeStruct((2, 4, BLK, HOME, COL), BF),
        grid=BLK,
        vmem=SMALL,
    )


def weights_kernel(s_ref, x_ref, g_ref, own_ref, *out_refs):
    near = NZ // BLK
    blocks = [x_ref.at[:, :, b * near : (b + 1) * near] for b in range(BLK)]
    tok, cot = (jnp.concatenate([features(b, which, RB) for b in blocks], axis=0) for which in range(2))
    for k, out_ref in enumerate((own_ref, *out_refs)):
        owner = x_of(s_ref, k)
        grads = jnp.concatenate([g_ref[owner, b, :RB] for b in range(BLK)], axis=0)
        halves = []
        for b in range(BLK):
            packed = g_ref[owner, b, RB:PRE]
            halves += [packed, pltpu.roll(packed.astype(F32), HID, 1).astype(BF)]
        both = dot(grads, tok, 0, 0)
        down = dot(jnp.concatenate(halves, axis=0), cot, 0, 0)
        out_ref[: 2 * HID] = both.astype(out_ref.dtype)
        out_ref[2 * HID :] = down[:HID].astype(out_ref.dtype)


def weights(where, x, g):
    shape = (3 * HID, 4 * COL)
    return call(
        weights_kernel,
        where,
        (x, g),
        [full(2, 4, NZ, 2, CAP, COL), full(4, BLK, ACT, COL)],
        [full(*shape)] * 4,
        [jax.ShapeDtypeStruct(shape, F32)] + [jax.ShapeDtypeStruct(shape, BF)] * 3,
        flops=4 * 10**9,
    )


def assemble_kernel(s_ref, *refs):
    *parts, dg_ref, du_ref, dd_ref = refs
    for k, p_ref in enumerate(parts):
        for y in range(4):
            cols = pl.ds(pl.multiple_of((y * 4 + x_of(s_ref, -k)) * COL, COL), COL)
            here = slice(y * COL, (y + 1) * COL)
            dg_ref[0, :, cols] = p_ref[:HID, here].astype(F32)
            du_ref[0, :, cols] = p_ref[HID : 2 * HID, here].astype(F32)
            dd_ref[0, :, cols] = p_ref[2 * HID :, here].astype(F32)


def assemble(where, parts):
    shape = (1, HID, TP * COL)
    return call(
        assemble_kernel,
        where,
        parts,
        [full(3 * HID, 4 * COL)] * 4,
        [full(*shape)] * 3,
        [jax.ShapeDtypeStruct(shape, F32)] * 3,
        flops=10**9,
    )


def total_kernel(s_ref, p_ref, out_ref):
    half, sums = RB // 2, []
    for core in range(2):
        rows = p_ref[core, 0, 0].astype(F32)
        for y in range(1, 4):
            rows = rows + p_ref[core, y, 0].astype(F32)
        out_ref[:, core * CAP : (core + 1) * CAP] = rows[:half].astype(BF).reshape(NZ // BLK, CAP, COL)
        sums.append(one_sum(rows[half:]))
    extra = two_parts(jnp.where((iota((EXT, COL), 1) & 31) < 16, *sums)).astype(F32)
    for k in range(NZ // BLK):
        out_ref[k, 2 * CAP :] = jnp.broadcast_to(extra[k : k + 1], (DUP, COL)).astype(BF)


def total(where, part):
    return call(
        total_kernel,
        where,
        (part,),
        [pl.BlockSpec((2, 4, 1, HOME, COL), lambda i, s: (0, 0, i, 0, 0))],
        pl.BlockSpec((NZ // BLK, 2 * CAP + DUP, COL), lambda i, s: (i, 0, 0)),
        jax.ShapeDtypeStruct((NZ, 2 * CAP + DUP, COL), BF),
        grid=BLK,
        vmem=4 * 2**20,
    )


def combine_kernel(s_ref, ids_ref, w_ref, home_ref, tok_ref, route_ref):
    first, second, rank, _, chosen = routing(ids_ref)
    pick = jnp.where(chosen, 1.0, 0.0).astype(BF)
    rows = home_ref[:, : 2 * CAP].reshape(2 * NZ * CAP, COL)
    tok_ref[...] = dot(pick, rows, 0, 0).astype(BF)
    sums = home_ref[:, 2 * CAP :].reshape(NZ * DUP, COL)
    row = iota((NZ * DUP, TOK), 0)
    lane = iota((COL, TOK), 0)
    w = w_ref[...].astype(F32)
    for k, member in enumerate((first, second)):
        ids = ids_ref[k : k + 1, :]
        at = jnp.sum(member * rank, axis=0, keepdims=True).astype(I32) + 16 * (ids & 1)
        chip = (((row & 7) == 0) & ((row >> 3) == (ids >> 1))).astype(BF)
        found = dot(sums, chip, 0, 0)
        found = jnp.where((lane == at) | (lane == at + 32), found, 0.0)
        route_ref[k : k + 1, :] = jnp.sum(found, axis=0, keepdims=True) / w[k : k + 1, :]


def combine(where, ids, w, home):
    return call(
        combine_kernel,
        where,
        (ids, w, home),
        [full(2, TOK), full(2, TOK), full(NZ, 2 * CAP + DUP, COL)],
        [full(TOK, COL), full(2, TOK)],
        [jax.ShapeDtypeStruct((TOK, COL), BF), jax.ShapeDtypeStruct((2, TOK), F32)],
        vmem=4 * 2**20,
    )


def exchange(x, axis):
    return lax.all_to_all(x, axis, split_axis=0, concat_axis=0, tiled=True)


def copies(x, n):
    return jnp.broadcast_to(x[None], (n, *x.shape))


def shifted(x, axis, by):
    n = lax.axis_size(axis)
    return lax.ppermute(x, axis, [(i, (i + by) % n) for i in range(n)])


def row_weights(where, wg, wu, wd):
    own, *others = pack(where, wg, wu, wd)
    moved = [shifted(other, "x", k + 1) for k, other in enumerate(others)]
    return layout(where, (own, *moved))


def per_device(tokens, cotangent, expert_ids, route_weight, gate_weight, up_weight, down_weight):
    y, x = lax.axis_index("y"), lax.axis_index("x")
    where = jnp.stack([y * 4 + x, x]).astype(I32)
    ids, w = expert_ids.T, route_weight.T
    mine = exchange(dispatch(where, ids, w, tokens, cotangent), "z")
    wgu, wdd = row_weights(where, gate_weight, up_weight, down_weight)
    both = copies(mine.transpose(1, 0, 2, 3, 4), 4).transpose(1, 0, 2, 3, 4, 5)
    rows = exchange(both.reshape(8, NZ, 2, CAP, COL), ("c", "y")).reshape(both.shape)
    pre = pre_activations(where, rows, wgu, wdd)
    pre = exchange(pre, "x")
    g = activations(where, pre)
    g = exchange(g, "x")
    part = back(where, g, wgu)
    sums = exchange(part.reshape(8, BLK, HOME, COL), ("c", "y")).reshape(part.shape)
    kept, *sent = weights(where, rows, g)
    home = exchange(total(where, sums), "z")
    moved = [shifted(part, "x", k + 1) for k, part in enumerate(sent)]
    gate_grad, up_grad, down_grad = assemble(where, (kept, *moved))
    tokens_grad, route_grad = combine(where, ids, w, home)
    return tokens_grad, route_grad.T, gate_grad, up_grad, down_grad


def solution(mesh):
    grid = Mesh(mesh.devices.reshape(NZ, 2, 4, 4), ("z", "c", "y", "x"))
    ep, tp = ("z", "c"), ("y", "x")
    weight = P(ep, tp, None)
    return jax.shard_map(
        per_device,
        mesh=grid,
        in_specs=(P(ep, None), P(ep, None), P(ep, None), P(ep, None), weight, weight, weight),
        out_specs=(P(ep, tp), P(ep, None), weight, weight, weight),
        check_vma=False,
    )
```

```python
import jax
import jax.numpy as jnp
from jax import lax
from jax.experimental import pallas as pl
from jax.experimental.pallas import tpu as pltpu
from jax.sharding import Mesh
from jax.sharding import PartitionSpec as P


GROUP = ("c", "y", "u")

BF = jnp.bfloat16
F32 = jnp.float32
I32 = jnp.int32
NZ = 16
TP = 16
TOK = 128
CAP = 16
COL = 128
HALF = 8
HID = 64
ROWS = 512
BLK = 2
RB = ROWS // BLK
SMALL = 12 * 2**20
EXT = 2 * NZ // BLK
DUP = 8


def iota(shape, dim):
    return lax.broadcasted_iota(I32, shape, dim)


def dot(a, b, ca, cb, precision=None):
    return lax.dot_general(
        a, b, (((ca,), (cb,)), ((), ())), precision=precision, preferred_element_type=F32
    )


def routing(ids_ref):
    experts = 2 * NZ
    row = iota((experts, TOK), 0)
    first = (ids_ref[0:1, :] == row).astype(F32)
    second = (ids_ref[1:2, :] == row).astype(F32)
    member = first + second
    earlier = (iota((TOK, TOK), 0) < iota((TOK, TOK), 1)).astype(BF)
    rank = dot(member.astype(BF), earlier, 1, 0)
    slots = experts * CAP
    expand = ((iota((slots, experts), 0) >> 4) == iota((slots, experts), 1)).astype(BF)
    hit = dot(expand, member.astype(BF), 1, 0)
    at = dot(expand, rank.astype(BF), 1, 0)
    place = (iota((slots, TOK), 0) & 15).astype(F32)
    chosen = (hit > 0.5) & (at == place)
    return first, second, rank, expand, chosen


def dispatch_kernel(s_ref, ids_ref, w_ref, tok_ref, cot_ref, out_ref):
    first, second, _, expand, chosen = routing(ids_ref)
    w = w_ref[...].astype(F32)
    weighted = first * w[0:1, :] + second * w[1:2, :]
    scale = dot(expand, weighted.astype(BF), 1, 0)
    pick = jnp.where(chosen, 1.0, 0.0).astype(BF)
    pick_scaled = jnp.where(chosen, scale, 0.0).astype(BF)
    out_ref[:, :, 0] = dot(pick, tok_ref[...], 1, 0).astype(BF).reshape(NZ, 2, CAP, COL)
    out_ref[:, :, 1] = dot(pick_scaled, cot_ref[...], 1, 0).astype(BF).reshape(NZ, 2, CAP, COL)


def dispatch(where, ids, w, tokens, cotangent):
    mine = pl.BlockSpec((TOK, COL), lambda i, s: (0, s[0]))
    return call(
        dispatch_kernel,
        where,
        (ids, w, tokens, cotangent),
        [full(2, TOK), full(2, TOK), mine, mine],
        full(NZ, 2, 2, CAP, COL),
        jax.ShapeDtypeStruct((NZ, 2, 2, CAP, COL), BF),
    )


def cols(q):
    return slice(q * COL, (q + 1) * COL)


def block(q, v):
    j = (q >> 1) * 4 + (q & 1) * 2 + v
    return pl.ds(pl.multiple_of(j * COL, COL), COL)


def full(*shape):
    return pl.BlockSpec(shape, lambda i, s: (0,) * len(shape))


def call(kernel, where, args, in_specs, out_specs, out_shape, scratch=(), grid=1, flops=10**8, vmem=None):
    return pl.pallas_call(
        kernel,
        grid_spec=pltpu.PrefetchScalarGridSpec(
            num_scalar_prefetch=1,
            grid=(grid,),
            in_specs=in_specs,
            out_specs=out_specs,
            scratch_shapes=list(scratch),
        ),
        out_shape=out_shape,
        compiler_params=pltpu.CompilerParams(vmem_limit_bytes=vmem),
        cost_estimate=pl.CostEstimate(flops=flops, bytes_accessed=2 * 10**6, transcendentals=0),
    )(where, *args)


def pack_kernel(s_ref, wg_ref, wu_ref, wd_ref, out_ref):
    for i, w_ref in enumerate((wg_ref, wu_ref, wd_ref)):
        for q in range(HALF):
            out_ref[i, :, cols(q)] = w_ref[0, :, block(q, 1 - s_ref[1])]


def pack(where, ws):
    shape = (3, HID, HALF * COL)
    return call(
        pack_kernel,
        where,
        ws,
        [full(1, HID, TP * COL)] * 3,
        full(*shape),
        jax.ShapeDtypeStruct(shape, BF),
    )


def layout_kernel(s_ref, wg_ref, wu_ref, wd_ref, got_ref, up_ref, down_ref):
    v = s_ref[1]
    for i, w_ref in enumerate((wg_ref, wu_ref, wd_ref)):
        to_ref, at = (up_ref, i * 2 * HID) if i < 2 else (down_ref, 0)
        mine = pl.ds(pl.multiple_of(at + v * HID, HID), HID)
        theirs = pl.ds(pl.multiple_of(at + (1 - v) * HID, HID), HID)
        to_ref[theirs, :] = got_ref[i]
        for q in range(HALF):
            to_ref[mine, cols(q)] = w_ref[0, :, block(q, v)]


def layout(where, ws, got):
    d = HALF * COL
    return call(
        layout_kernel,
        where,
        (*ws, got),
        [full(1, HID, TP * COL)] * 3 + [full(3, HID, d)],
        [full(4 * HID, d), full(2 * HID, d)],
        [jax.ShapeDtypeStruct((4 * HID, d), BF), jax.ShapeDtypeStruct((2 * HID, d), BF)],
        vmem=SMALL,
    )


def features(x_ref, which, rows):
    pieces = [x_ref[:, q >> 1, q & 1, :, which].reshape(rows, COL) for q in range(HALF)]
    return jnp.concatenate(pieces, axis=1)


def pre_kernel(s_ref, x_ref, up_ref, down_ref, kept_ref, sent_ref):
    pre = dot(features(x_ref, 0, RB), up_ref[...], 1, 1)
    back = dot(features(x_ref, 1, RB), down_ref[...], 1, 1)
    for i, part in enumerate((pre[:, :COL], pre[:, COL:], back)):
        kept_ref[0, i] = part
        sent_ref[0, i] = part.astype(BF)


THREE = (BLK, 3, RB, COL)
HOME = RB // 2 + EXT


def three():
    return pl.BlockSpec((1, 3, RB, COL), lambda i, s: (i, 0, 0, 0))


def pre_activations(where, x, up, down):
    d = HALF * COL
    return call(
        pre_kernel,
        where,
        (x, up, down),
        [
            pl.BlockSpec((2, 4, 2, NZ // BLK, 2, CAP, COL), lambda i, s: (0, 0, 0, i, 0, 0, 0)),
            full(4 * HID, d),
            full(2 * HID, d),
        ],
        [three(), three()],
        [jax.ShapeDtypeStruct(THREE, F32), jax.ShapeDtypeStruct(THREE, BF)],
        grid=BLK,
        vmem=SMALL,
    )


def two_parts(sums):
    high = sums.astype(BF).astype(F32)
    return jnp.where(iota((EXT, COL), 1) < 32, high, sums - high).astype(BF)


def one_sum(parts):
    both = parts + pltpu.roll(parts, COL - 32, 1)
    low = iota((EXT, COL), 1) < 32
    both = jnp.where(low, both, 0.0)
    return both + pltpu.roll(both, 32, 1)


def act_kernel(s_ref, kept_ref, got_ref, up_ref, out_ref, act_ref):
    gate, up, back = (kept_ref[0, i] + got_ref[0, i].astype(F32) for i in range(3))
    sigma = 1.0 / (1.0 + jnp.exp(-gate))
    silu = gate * sigma
    hidden = silu * up
    grad_gate = (back * up * sigma * (1.0 + gate * (1.0 - sigma))).astype(BF)
    grad_up = (back * silu).astype(BF)
    act_ref[0, 0] = grad_gate
    act_ref[0, 1] = grad_up
    act_ref[0, 2] = hidden.astype(BF)
    total = jnp.sum(hidden * back, axis=1, keepdims=True)
    spread = jnp.where((iota((RB, COL), 1) & 15) == (iota((RB, COL), 0) & 15), total, 0.0)
    group = (iota((EXT, RB), 0) == (iota((EXT, RB), 1) >> 4)).astype(F32)
    sums = dot(group, spread, 1, 0, lax.Precision.HIGHEST)
    pieces = dot(jnp.concatenate([grad_gate, grad_up], axis=1), up_ref[...], 1, 0).astype(BF)
    half = RB // 2
    for core in range(2):
        extra = two_parts(sums if core == 0 else pltpu.roll(sums, EXT // 2, 0))
        for q in range(HALF):
            out_ref[core, q, 0, :half] = pieces[core * half : (core + 1) * half, cols(q)]
            out_ref[core, q, 0, half:] = extra


def activations(where, kept, got, up):
    shape = (2, HALF, BLK, HOME, COL)
    return call(
        act_kernel,
        where,
        (kept, got, up),
        [three(), three(), full(4 * HID, HALF * COL)],
        [pl.BlockSpec((2, HALF, 1, HOME, COL), lambda i, s: (0, 0, i, 0, 0)), three()],
        [jax.ShapeDtypeStruct(shape, BF), jax.ShapeDtypeStruct(THREE, BF)],
        grid=BLK,
        vmem=SMALL,
    )


def weights_kernel(s_ref, x_ref, act_ref, kept_ref, sent_ref):
    near = NZ // BLK
    blocks = [x_ref.at[:, :, :, b * near : (b + 1) * near] for b in range(BLK)]
    tok, cot = (jnp.concatenate([features(b, which, RB) for b in blocks], axis=0) for which in range(2))
    first = s_ref[1] == 0
    for i, rows in enumerate((tok, tok, cot)):
        act = jnp.concatenate([act_ref[b, i] for b in range(BLK)], axis=0)
        both = dot(act, rows, 0, 0)
        here = slice(i * HID, (i + 1) * HID)
        kept_ref[here] = jnp.where(first, both[:HID], both[HID:])
        sent_ref[here] = jnp.where(first, both[HID:], both[:HID]).astype(BF)


def weights(where, x, act):
    shape = (3 * HID, HALF * COL)
    return call(
        weights_kernel,
        where,
        (x, act),
        [full(2, 4, 2, NZ, 2, CAP, COL), full(*THREE)],
        [full(*shape)] * 2,
        [jax.ShapeDtypeStruct(shape, F32), jax.ShapeDtypeStruct(shape, BF)],
        flops=4 * 10**9,
    )


def assemble_kernel(s_ref, kept_ref, got_ref, *out_refs):
    v = s_ref[1]
    for i, out_ref in enumerate(out_refs):
        here = slice(i * HID, (i + 1) * HID)
        for q in range(HALF):
            out_ref[0, :, block(q, v)] = kept_ref[here, cols(q)]
            out_ref[0, :, block(q, 1 - v)] = got_ref[here, cols(q)].astype(F32)


def assemble(where, kept, got):
    shape = (1, HID, TP * COL)
    return call(
        assemble_kernel,
        where,
        (kept, got),
        [full(3 * HID, HALF * COL)] * 2,
        [full(*shape)] * 3,
        [jax.ShapeDtypeStruct(shape, F32)] * 3,
        flops=10**9,
    )


def total_kernel(s_ref, p_ref, out_ref):
    half, sums = RB // 2, []
    for core in range(2):
        rows = p_ref[core, 0, 0].astype(F32)
        for q in range(1, HALF):
            rows = rows + p_ref[core, q, 0].astype(F32)
        out_ref[:, core * CAP : (core + 1) * CAP] = rows[:half].astype(BF).reshape(NZ // BLK, CAP, COL)
        sums.append(one_sum(rows[half:]))
    extra = two_parts(jnp.where((iota((EXT, COL), 1) & 31) < 16, *sums)).astype(F32)
    for k in range(NZ // BLK):
        out_ref[k, 2 * CAP :] = jnp.broadcast_to(extra[k : k + 1], (DUP, COL)).astype(BF)


def total(where, part):
    return call(
        total_kernel,
        where,
        (part,),
        [pl.BlockSpec((2, HALF, 1, HOME, COL), lambda i, s: (0, 0, i, 0, 0))],
        pl.BlockSpec((NZ // BLK, 2 * CAP + DUP, COL), lambda i, s: (i, 0, 0)),
        jax.ShapeDtypeStruct((NZ, 2 * CAP + DUP, COL), BF),
        grid=BLK,
        vmem=8 * 2**20,
    )


def combine_kernel(s_ref, ids_ref, w_ref, home_ref, tok_ref, route_ref):
    first, second, rank, _, chosen = routing(ids_ref)
    pick = jnp.where(chosen, 1.0, 0.0).astype(BF)
    rows = home_ref[:, : 2 * CAP].reshape(2 * NZ * CAP, COL)
    tok_ref[...] = dot(pick, rows, 0, 0).astype(BF)
    sums = home_ref[:, 2 * CAP :].reshape(NZ * DUP, COL)
    row = iota((NZ * DUP, TOK), 0)
    lane = iota((COL, TOK), 0)
    w = w_ref[...].astype(F32)
    for k, member in enumerate((first, second)):
        ids = ids_ref[k : k + 1, :]
        at = jnp.sum(member * rank, axis=0, keepdims=True).astype(I32) + 16 * (ids & 1)
        chip = (((row & 7) == 0) & ((row >> 3) == (ids >> 1))).astype(BF)
        found = dot(sums, chip, 0, 0)
        found = jnp.where((lane == at) | (lane == at + 32), found, 0.0)
        route_ref[k : k + 1, :] = jnp.sum(found, axis=0, keepdims=True) / w[k : k + 1, :]


def combine(where, ids, w, home):
    return call(
        combine_kernel,
        where,
        (ids, w, home),
        [full(2, TOK), full(2, TOK), full(NZ, 2 * CAP + DUP, COL)],
        [full(TOK, COL), full(2, TOK)],
        [jax.ShapeDtypeStruct((TOK, COL), BF), jax.ShapeDtypeStruct((2, TOK), F32)],
        vmem=4 * 2**20,
    )


def exchange(x, axis):
    return lax.all_to_all(x, axis, split_axis=0, concat_axis=0, tiled=True)


def copies(x, n):
    return jnp.broadcast_to(x[None], (n, *x.shape))


def swapped(x):
    return lax.ppermute(x, "v", [(0, 1), (1, 0)])


def row_weights(where, ws):
    sent = pack(where, ws)
    got = swapped(sent)
    return layout(where, ws, got)


def per_device(tokens, cotangent, expert_ids, route_weight, *ws):
    y, u, v = (lax.axis_index(axis) for axis in GROUP[1:] + ("v",))
    where = jnp.stack([y * 4 + u * 2 + v, v]).astype(I32)
    ids, w = expert_ids.T, route_weight.T
    mine = exchange(dispatch(where, ids, w, tokens, cotangent), "z")
    up, down = row_weights(where, ws)
    both = copies(mine.transpose(1, 0, 2, 3, 4), HALF).transpose(1, 0, 2, 3, 4, 5)
    rows = exchange(both.reshape(2 * HALF, NZ, 2, CAP, COL), GROUP)
    rows = rows.reshape(2, 4, 2, NZ, 2, CAP, COL)
    kept, sent = pre_activations(where, rows, up, down)
    got = swapped(sent)
    part, act = activations(where, kept, got, up)
    sums = exchange(part.reshape(2 * HALF, BLK, HOME, COL), GROUP).reshape(part.shape)
    kept, sent = weights(where, rows, act)
    home = exchange(total(where, sums), "z")
    got = swapped(sent)
    gate_grad, up_grad, down_grad = assemble(where, kept, got)
    tokens_grad, route_grad = combine(where, ids, w, home)
    return tokens_grad, route_grad.T, gate_grad, up_grad, down_grad


def solution(mesh):
    grid = Mesh(mesh.devices.reshape(NZ, 2, 4, 2, 2), ("z", "c", "y", "u", "v"))
    ep, tp = ("z", "c"), ("y", "u", "v")
    weight = P(ep, tp, None)
    return jax.shard_map(
        per_device,
        mesh=grid,
        in_specs=(P(ep, None), P(ep, None), P(ep, None), P(ep, None), weight, weight, weight),
        out_specs=(P(ep, tp), P(ep, None), weight, weight, weight),
        check_vma=False,
    )
```

```python
import jax
import jax.numpy as jnp
from jax import lax
from jax.experimental import pallas as pl
from jax.experimental.pallas import tpu as pltpu
from jax.sharding import Mesh
from jax.sharding import PartitionSpec as P


BF = jnp.bfloat16
F32 = jnp.float32
I32 = jnp.int32
NZ = 16
TP = 16
TOK = 128
CAP = 16
COL = 128
HID = 64
ROWS = 512
BLK = 2
RB = ROWS // BLK
SMALL = 12 * 2**20
EXT = 2 * NZ // BLK
DUP = 8


def iota(shape, dim):
    return lax.broadcasted_iota(I32, shape, dim)


def dot(a, b, ca, cb, precision=None):
    return lax.dot_general(
        a, b, (((ca,), (cb,)), ((), ())), precision=precision, preferred_element_type=F32
    )


def routing(ids_ref):
    experts = 2 * NZ
    row = iota((experts, TOK), 0)
    first = (ids_ref[0:1, :] == row).astype(F32)
    second = (ids_ref[1:2, :] == row).astype(F32)
    member = first + second
    earlier = (iota((TOK, TOK), 0) < iota((TOK, TOK), 1)).astype(BF)
    rank = dot(member.astype(BF), earlier, 1, 0)
    slots = experts * CAP
    expand = ((iota((slots, experts), 0) >> 4) == iota((slots, experts), 1)).astype(BF)
    hit = dot(expand, member.astype(BF), 1, 0)
    at = dot(expand, rank.astype(BF), 1, 0)
    place = (iota((slots, TOK), 0) & 15).astype(F32)
    chosen = (hit > 0.5) & (at == place)
    return first, second, rank, expand, chosen


def dispatch_kernel(s_ref, ids_ref, w_ref, tok_ref, cot_ref, own_ref, other_ref):
    first, second, _, expand, chosen = routing(ids_ref)
    w = w_ref[...].astype(F32)
    weighted = first * w[0:1, :] + second * w[1:2, :]
    scale = dot(expand, weighted.astype(BF), 1, 0)
    pick = jnp.where(chosen, 1.0, 0.0).astype(BF)
    pick_scaled = jnp.where(chosen, scale, 0.0).astype(BF)
    first_core = s_ref[1] == 0
    for i, rows in enumerate((dot(pick, tok_ref[...], 1, 0), dot(pick_scaled, cot_ref[...], 1, 0))):
        rows = rows.reshape(NZ, 2, CAP, COL)
        own_ref[:, i] = jnp.where(first_core, rows[:, 0], rows[:, 1]).astype(BF)
        other_ref[:, i] = jnp.where(first_core, rows[:, 1], rows[:, 0]).astype(BF)


def dispatch(where, ids, w, tokens, cotangent):
    mine = pl.BlockSpec((TOK, COL), lambda i, s: (0, s[0]))
    return call(
        dispatch_kernel,
        where,
        (ids, w, tokens, cotangent),
        [full(2, TOK), full(2, TOK), mine, mine],
        [full(NZ, 2, CAP, COL)] * 2,
        [jax.ShapeDtypeStruct((NZ, 2, CAP, COL), BF)] * 2,
    )


def b_of(s_ref, k):
    return (s_ref[2] + k) & 3


def block(s_ref, a, b):
    j = jnp.where(s_ref[1] == 0, a * 4 + b, b * 4 + a)
    return pl.ds(pl.multiple_of(j * COL, COL), COL)


def pack_kernel(s_ref, wg_ref, wu_ref, wd_ref, *out_refs):
    for k, out_ref in enumerate(out_refs):
        for y in range(4):
            cols = block(s_ref, y, b_of(s_ref, k))
            out_ref[y, :HID] = wg_ref[0, :, cols]
            out_ref[y, HID : 2 * HID] = wu_ref[0, :, cols]
            out_ref[y, 2 * HID :] = wd_ref[0, :, cols]


def full(*shape):
    return pl.BlockSpec(shape, lambda i, s: (0,) * len(shape))


def call(kernel, where, args, in_specs, out_specs, out_shape, scratch=(), grid=1, flops=10**8, vmem=None):
    return pl.pallas_call(
        kernel,
        grid_spec=pltpu.PrefetchScalarGridSpec(
            num_scalar_prefetch=1,
            grid=(grid,),
            in_specs=in_specs,
            out_specs=out_specs,
            scratch_shapes=list(scratch),
        ),
        out_shape=out_shape,
        compiler_params=pltpu.CompilerParams(vmem_limit_bytes=vmem),
        cost_estimate=pl.CostEstimate(flops=flops, bytes_accessed=2 * 10**6, transcendentals=0),
    )(where, *args)


def pack(where, wg, wu, wd):
    shape = (4, 3 * HID, COL)
    return call(
        pack_kernel,
        where,
        (wg, wu, wd),
        [full(1, HID, TP * COL)] * 3,
        [full(*shape)] * 4,
        [jax.ShapeDtypeStruct(shape, BF)] * 4,
    )


def low_lanes(rows):
    return iota((rows, COL), 1) < HID


def features(x_ref, which, rows):
    return jnp.concatenate([x_ref[y, :, :, which].reshape(rows, COL) for y in range(4)], axis=1)


def layout_kernel(s_ref, w0_ref, w1_ref, w2_ref, w3_ref, wgu_ref, wdd_ref):
    for k, w_ref in enumerate((w0_ref, w1_ref, w2_ref, w3_ref)):
        for y in range(4):
            cols = slice(y * COL, (y + 1) * COL)
            wgu_ref[k * COL : (k + 1) * COL, cols] = w_ref[y, : 2 * HID]
            wdd_ref[k * COL : k * COL + HID, cols] = w_ref[y, 2 * HID :]
            wdd_ref[k * COL + HID : (k + 1) * COL, cols] = w_ref[y, 2 * HID :]


def layout(where, ws):
    shape = (4 * COL, 4 * COL)
    return call(
        layout_kernel,
        where,
        ws,
        [full(4, 3 * HID, COL)] * 4,
        [full(*shape)] * 2,
        [jax.ShapeDtypeStruct(shape, BF)] * 2,
        vmem=SMALL,
    )


def pre_kernel(s_ref, x_ref, wgu_ref, wdd_ref, out_ref):
    pre = dot(features(x_ref, 0, RB), wgu_ref[...], 1, 1).astype(BF)
    back = dot(features(x_ref, 1, RB), wdd_ref[...], 1, 1)
    for k in range(4):
        cols = slice(k * COL, (k + 1) * COL)
        to = b_of(s_ref, -k)
        half = back[:, cols]
        out_ref[to, 0, :RB] = pre[:, cols]
        out_ref[to, 0, RB:] = jnp.where(low_lanes(RB // 2), half[: RB // 2], half[RB // 2 :]).astype(BF)


PRE = RB + RB // 2
ACT = PRE + EXT


def pre_activations(where, x, wgu, wdd):
    return call(
        pre_kernel,
        where,
        (x, wgu, wdd),
        [
            pl.BlockSpec((4, NZ // BLK, 2, 2, CAP, COL), lambda i, s: (0, i, 0, 0, 0, 0)),
            full(4 * COL, 4 * COL),
            full(4 * COL, 4 * COL),
        ],
        pl.BlockSpec((4, 1, PRE, COL), lambda i, s: (0, i, 0, 0)),
        jax.ShapeDtypeStruct((4, BLK, PRE, COL), BF),
        grid=BLK,
        vmem=SMALL,
    )


def act_kernel(s_ref, p_ref, g_ref):
    sums = p_ref[0, 0].astype(F32)
    for x in range(1, 4):
        sums = sums + p_ref[x, 0].astype(F32)
    pre, packed = sums[:RB], sums[RB:]
    low = low_lanes(RB // 2)
    other = pltpu.roll(packed, HID, 1)
    back = jnp.concatenate([jnp.where(low, packed, other), jnp.where(low, other, packed)], axis=0)
    lane = iota((RB, COL), 1)
    low_half = lane < HID
    turned = pltpu.roll(pre, HID, 1)
    gate = jnp.where(low_half, pre, turned)
    up = jnp.where(low_half, turned, pre)
    sigma = 1.0 / (1.0 + jnp.exp(-gate))
    silu = gate * sigma
    hidden = silu * up
    grads = jnp.where(low_half, back * up * sigma * (1.0 + gate * (1.0 - sigma)), back * silu).astype(BF)
    weighted = jnp.where(low, hidden[: RB // 2], hidden[RB // 2 :]).astype(BF)
    total = jnp.sum(jnp.where(low_half, hidden * back, 0.0), axis=1, keepdims=True)
    spread = jnp.where((lane & 15) == (iota((RB, COL), 0) & 15), total, 0.0)
    group = (iota((EXT, RB), 0) == (iota((EXT, RB), 1) >> 4)).astype(F32)
    extra = two_parts(dot(group, spread, 1, 0, lax.Precision.HIGHEST))
    for x in range(4):
        g_ref[x, 0, :RB] = grads
        g_ref[x, 0, RB:PRE] = weighted
        g_ref[x, 0, PRE:] = extra


def activations(where, p):
    return call(
        act_kernel,
        where,
        (p,),
        [pl.BlockSpec((4, 1, PRE, COL), lambda i, s: (0, i, 0, 0))],
        pl.BlockSpec((4, 1, ACT, COL), lambda i, s: (0, i, 0, 0)),
        jax.ShapeDtypeStruct((4, BLK, ACT, COL), BF),
        grid=BLK,
        vmem=SMALL,
    )


def two_parts(sums):
    high = sums.astype(BF).astype(F32)
    return jnp.where(iota((EXT, COL), 1) < 32, high, sums - high).astype(BF)


def one_sum(parts):
    both = parts + pltpu.roll(parts, COL - 32, 1)
    low = iota((EXT, COL), 1) < 32
    both = jnp.where(low, both, 0.0)
    return both + pltpu.roll(both, 32, 1)


def back_kernel(s_ref, g_ref, w_ref, out_ref):
    grads = jnp.concatenate([g_ref[b_of(s_ref, -k), 0, :RB] for k in range(4)], axis=1)
    pieces = dot(grads, w_ref[...], 1, 0).astype(BF)
    parts = g_ref[0, 0, PRE:].astype(F32)
    for x in range(1, 4):
        parts = parts + g_ref[x, 0, PRE:].astype(F32)
    extra = two_parts(one_sum(parts))
    for y in range(4):
        out_ref[y, 0, :RB] = pieces[:, y * COL : (y + 1) * COL]
        out_ref[y, 0, RB:] = extra


def back(where, g, w):
    return call(
        back_kernel,
        where,
        (g, w),
        [pl.BlockSpec((4, 1, ACT, COL), lambda i, s: (0, i, 0, 0)), full(4 * COL, 4 * COL)],
        pl.BlockSpec((4, 1, RB + EXT, COL), lambda i, s: (0, i, 0, 0)),
        jax.ShapeDtypeStruct((4, BLK, RB + EXT, COL), BF),
        grid=BLK,
        vmem=SMALL,
    )


def weights_kernel(s_ref, x_ref, g_ref, own_ref, *out_refs):
    near = NZ // BLK
    blocks = [x_ref.at[:, b * near : (b + 1) * near] for b in range(BLK)]
    tok, cot = (jnp.concatenate([features(b, which, RB) for b in blocks], axis=0) for which in range(2))
    for k, out_ref in enumerate((own_ref, *out_refs)):
        owner = b_of(s_ref, k)
        grads = jnp.concatenate([g_ref[owner, b, :RB] for b in range(BLK)], axis=0)
        halves = []
        for b in range(BLK):
            packed = g_ref[owner, b, RB:PRE]
            halves += [packed, pltpu.roll(packed.astype(F32), HID, 1).astype(BF)]
        both = dot(grads, tok, 0, 0)
        down = dot(jnp.concatenate(halves, axis=0), cot, 0, 0)
        out_ref[: 2 * HID] = both.astype(out_ref.dtype)
        out_ref[2 * HID :] = down[:HID].astype(out_ref.dtype)


def weights(where, x, g):
    shape = (3 * HID, 4 * COL)
    return call(
        weights_kernel,
        where,
        (x, g),
        [full(4, NZ, 2, 2, CAP, COL), full(4, BLK, ACT, COL)],
        [full(*shape)] * 4,
        [jax.ShapeDtypeStruct(shape, F32)] + [jax.ShapeDtypeStruct(shape, BF)] * 3,
        flops=4 * 10**9,
    )


def assemble_kernel(s_ref, *refs):
    *parts, dg_ref, du_ref, dd_ref = refs
    for k, p_ref in enumerate(parts):
        for y in range(4):
            cols = block(s_ref, y, b_of(s_ref, -k))
            here = slice(y * COL, (y + 1) * COL)
            dg_ref[0, :, cols] = p_ref[:HID, here].astype(F32)
            du_ref[0, :, cols] = p_ref[HID : 2 * HID, here].astype(F32)
            dd_ref[0, :, cols] = p_ref[2 * HID :, here].astype(F32)


def assemble(where, parts):
    shape = (1, HID, TP * COL)
    return call(
        assemble_kernel,
        where,
        parts,
        [full(3 * HID, 4 * COL)] * 4,
        [full(*shape)] * 3,
        [jax.ShapeDtypeStruct(shape, F32)] * 3,
        flops=10**9,
    )


def total_kernel(s_ref, p_ref, out_ref):
    rows = p_ref[0, 0].astype(F32)
    for y in range(1, 4):
        rows = rows + p_ref[y, 0].astype(F32)
    near = NZ // BLK
    out_ref[:, : 2 * CAP] = rows[:RB].astype(BF).reshape(near, 2 * CAP, COL)
    sums = two_parts(one_sum(rows[RB:])).astype(F32)
    left = (iota((DUP, COL), 1) & 31) < 16
    for k in range(near):
        pair = [jnp.broadcast_to(sums[i : i + 1], (DUP, COL)) for i in (2 * k, 2 * k + 1)]
        out_ref[k, 2 * CAP :] = jnp.where(left, *pair).astype(BF)


def total(where, part):
    return call(
        total_kernel,
        where,
        (part,),
        [pl.BlockSpec((4, 1, RB + EXT, COL), lambda i, s: (0, i, 0, 0))],
        pl.BlockSpec((NZ // BLK, 2 * CAP + DUP, COL), lambda i, s: (i, 0, 0)),
        jax.ShapeDtypeStruct((NZ, 2 * CAP + DUP, COL), BF),
        grid=BLK,
        vmem=4 * 2**20,
    )


def combine_kernel(s_ref, ids_ref, w_ref, home_ref, far_ref, tok_ref, route_ref):
    core = s_ref[1]
    first, second, rank, _, chosen = routing(ids_ref)
    pick = jnp.where(chosen, 1.0, 0.0).astype(BF)
    home, far = home_ref[:, :CAP], far_ref[:, :CAP]
    low = jnp.where(core == 0, home, far)
    high = jnp.where(core == 0, far, home)
    rows = jnp.concatenate([low, high], axis=1).reshape(2 * NZ * CAP, COL)
    tok_ref[...] = dot(pick, rows, 0, 0).astype(BF)
    home_sums = home_ref[:, 2 * CAP :].reshape(NZ * DUP, COL)
    far_sums = far_ref[:, CAP:].reshape(NZ * DUP, COL)
    row = iota((NZ * DUP, TOK), 0)
    leads, chip = (row & 7) == 0, row >> 3
    lane = iota((COL, TOK), 0)
    w = w_ref[...].astype(F32)
    for k, member in enumerate((first, second)):
        ids = ids_ref[k : k + 1, :]
        at = jnp.sum(member * rank, axis=0, keepdims=True).astype(I32)
        near = dot(home_sums, (leads & (ids == 2 * chip + core)).astype(BF), 0, 0)
        away = dot(far_sums, (leads & (ids == 2 * chip + 1 - core)).astype(BF), 0, 0)
        near = jnp.where((lane == at) | (lane == at + 32), near, 0.0)
        away = jnp.where((lane == at + 16) | (lane == at + 48), away, 0.0)
        route_ref[k : k + 1, :] = jnp.sum(near + away, axis=0, keepdims=True) / w[k : k + 1, :]


def combine(where, ids, w, home, far):
    return call(
        combine_kernel,
        where,
        (ids, w, home, far),
        [
            full(2, TOK),
            full(2, TOK),
            full(NZ, 2 * CAP + DUP, COL),
            full(NZ, CAP + DUP, COL),
        ],
        [full(TOK, COL), full(2, TOK)],
        [jax.ShapeDtypeStruct((TOK, COL), BF), jax.ShapeDtypeStruct((2, TOK), F32)],
        vmem=4 * 2**20,
    )


PLANE = ("c", "y", "x")


def device(core, a, b):
    return core * 16 + (a * 4 + b if core == 0 else b * 4 + a)


def lines(first):
    places = [[(a, b) if first else (b, a) for a in range(4)] for b in range(4)]
    return [[device(core, a, b) for a, b in line] for core in range(2) for line in places]


def exchange(x, axis):
    return lax.all_to_all(x, axis, split_axis=0, concat_axis=0, tiled=True)


def line_exchange(x, first):
    return lax.all_to_all(
        x, PLANE, split_axis=0, concat_axis=0, tiled=True, axis_index_groups=lines(first)
    )


def shifted(x, by):
    pairs = [
        (device(core, a, b), device(core, a, (b + by) % 4))
        for core in range(2)
        for a in range(4)
        for b in range(4)
    ]
    return lax.ppermute(x, PLANE, pairs)


def swapped(x):
    return lax.ppermute(x, "c", [(0, 1), (1, 0)])


def copies(x, n):
    return jnp.broadcast_to(x[None], (n, *x.shape))


def row_weights(where, wg, wu, wd):
    own, *others = pack(where, wg, wu, wd)
    moved = [shifted(other, k + 1) for k, other in enumerate(others)]
    return layout(where, (own, *moved))


def per_device(tokens, cotangent, expert_ids, route_weight, gate_weight, up_weight, down_weight):
    y, x, core = lax.axis_index("y"), lax.axis_index("x"), lax.axis_index("c")
    where = jnp.stack([y * 4 + x, core, jnp.where(core == 0, x, y)]).astype(I32)
    ids, w = expert_ids.T, route_weight.T
    own, other = dispatch(where, ids, w, tokens, cotangent)
    mine = jnp.stack([own, swapped(other)], axis=1)
    mine = exchange(mine, "z")
    wgu, wdd = row_weights(where, gate_weight, up_weight, down_weight)
    rows = line_exchange(copies(mine, 4), True)
    pre = pre_activations(where, rows, wgu, wdd)
    pre = line_exchange(pre, False)
    g = activations(where, pre)
    g = line_exchange(g, False)
    part = back(where, g, wgu)
    sums = line_exchange(part, True)
    kept, *sent = weights(where, rows, g)
    home = exchange(total(where, sums), "z")
    moved = []
    for k, part in enumerate(sent):
        moved.append(shifted(part, k + 1))
    gate_grad, up_grad, down_grad = assemble(where, (kept, *moved))
    far = swapped(home[:, CAP:])
    tokens_grad, route_grad = combine(where, ids, w, home, far)
    return tokens_grad, route_grad.T, gate_grad, up_grad, down_grad


def solution(mesh):
    grid = Mesh(mesh.devices.reshape(NZ, 2, 4, 4), ("z", "c", "y", "x"))
    ep, tp = ("z", "c"), ("y", "x")
    weight = P(ep, tp, None)
    return jax.shard_map(
        per_device,
        mesh=grid,
        in_specs=(P(ep, None), P(ep, None), P(ep, None), P(ep, None), weight, weight, weight),
        out_specs=(P(ep, tp), P(ep, None), weight, weight, weight),
        check_vma=False,
    )
```
